32 devices in a mesh: sp: 16 (over z, y, x), tp: 2 (over core).
Axes of the slice: x: 2, y: 2, z: 4, core: 2. Of those that a mesh axis runs over, the one named last changes fastest.
Arguments:
- queries: bfloat16 [3, 4096, 2048], P(None, 'sp', 'tp'), may hold values from -6 to 6
- keys: bfloat16 [3, 4096, 2048], P(None, 'sp', 'tp'), may hold values from -6 to 6
- values: bfloat16 [3, 4096, 2048], P(None, 'sp', 'tp'), may hold values from -6 to 6
- w_out: bfloat16 [2048, 2048], P(None, 'tp'), may hold values from -1 to 1
Outputs:
- mixed: bfloat16 [4096, 2048], P('sp', 'tp')
The draws below stay inside these ranges and needn't reach their ends.
All inputs are finite; a program needn't handle non-finite values.
Results may differ from the reference program's by a relative error of at most 0.01.
Values may be sent and summed in bfloat16 or wider, within the bound.
A program may use at most 128 MiB of HBM per device.

```python
from functools import partial
import jax
import jax.numpy as jnp
from jax import lax

D = 2048
HEADS = 16
HEAD = 128
GROUPS = 3
KEYS_PER_QUERY = 128
FIRST_STRIDE = 1
SECOND_STRIDE = 4
THIRD_STRIDE = 16
TOKENS = 4096


def planted_pair(key):
    base = jax.random.fold_in(key, 11)
    first_key, second_key, pick_key, sign_key = jax.random.split(base, 4)
    shape = (GROUPS, TOKENS, HEADS * HEAD)
    query_part = jnp.clip(jax.random.normal(first_key, shape, jnp.float32), -6.0, 6.0)
    key_part = jnp.clip(jax.random.normal(second_key, shape, jnp.float32), -6.0, 6.0)
    return (query_part, key_part)


def draw_queries(key, part):
    return planted_pair(key)[0].astype(jnp.bfloat16)


def draw_keys(key, part):
    return planted_pair(key)[1].astype(jnp.bfloat16)


def block_levels(stream_key, extent, cuts, least, top_value):
    gain = 1.0
    for axis_at, parts in cuts:
        steps = jax.random.uniform(jax.random.fold_in(jax.random.fold_in(stream_key, 6), axis_at), (parts,), jnp.float32, least / len(cuts), top_value / len(cuts))
        gain = gain * jnp.repeat(jnp.exp(steps), extent[axis_at] // parts).reshape((-1,) + (1,) * (len(extent) - 1 - axis_at))
    return gain


def bell_draw(key, extent, scale, bound, shards=(), held_as=jnp.bfloat16):
    values = jax.random.normal(key, extent, jnp.float32) * scale
    if len(shards) > 0:
        values = block_levels(key, extent, shards, -0.22, 0.18) * values
    return jnp.clip(values, min=-bound, max=bound).astype(held_as)


def setup_inputs(seed: int = 0) -> dict:
    splits = jax.random.split(jax.random.key(seed), 5)
    queries = draw_queries(jax.random.fold_in(splits[4], 71), 0)
    keys = draw_keys(jax.random.fold_in(splits[4], 71), 0)
    values = bell_draw(splits[2], (GROUPS, TOKENS, HEADS * HEAD), 1.0, 6.0, ((1, 16), (2, 2)))
    w_out = bell_draw(splits[3], (HEADS * HEAD, D), (HEADS * HEAD // 64) ** -0.5, 1.0, ((1, 2),))
    return {"queries": queries, "keys": keys, "values": values, "w_out": w_out}


ROPE_BASE = 10000.0
MASKED = -1e30


def turn_halves(matrix, cosine, sine_part):
    first_half, second_half = jnp.split(matrix, 2, axis=-1)
    return jnp.concatenate([first_half * cosine - second_half * sine_part,
                            second_half * cosine + first_half * sine_part], axis=-1)


def strided_head(triple, dilation):
    query_head, key_head, value_head = triple
    length = query_head.shape[0]
    block_count = length // (KEYS_PER_QUERY * dilation)

    def blocked(matrix):
        shaped = jnp.transpose(matrix.reshape(length // dilation, dilation, HEAD), (1, 0, 2))
        return shaped.reshape(dilation, block_count, KEYS_PER_QUERY, HEAD).astype(jnp.float32)

    def with_previous(matrix):
        shaped = blocked(matrix)
        earlier = jnp.concatenate([jnp.zeros_like(shaped[:, :1]), shaped[:, :-1]], axis=1)
        return jnp.concatenate([earlier, shaped], axis=2)

    q_blocks = blocked(query_head)
    key_blocks = with_previous(key_head)
    value_blocks = with_previous(value_head)
    scores = jnp.einsum("dnqe,dnke->dnqk", q_blocks, key_blocks, precision=lax.Precision.HIGHEST)
    q_index = jnp.arange(KEYS_PER_QUERY)[:, None]
    k_index = jnp.arange(2 * KEYS_PER_QUERY)[None, :]
    distance = q_index + KEYS_PER_QUERY - k_index
    band = (distance >= 0) & (distance <= KEYS_PER_QUERY)
    opening = (jnp.arange(block_count)[:, None, None] == 0) & (k_index[None] < KEYS_PER_QUERY)
    allowed = band[None] & jnp.logical_not(opening)
    scores = jnp.where(allowed[None], scores, MASKED)
    row_max = jnp.max(scores, axis=-1, keepdims=True)
    weights = jnp.exp(scores - row_max)
    row_sum = jnp.sum(weights, axis=-1, keepdims=True)
    rounded = lax.optimization_barrier(weights.astype(jnp.bfloat16)).astype(jnp.float32)
    weighted = jnp.einsum("dnqk,dnke->dnqe", rounded, value_blocks, precision=lax.Precision.HIGHEST)
    result = weighted / row_sum
    log_sum = (row_max + jnp.log(row_sum))[..., 0]
    result = jnp.transpose(result.reshape(dilation, length // dilation, HEAD), (1, 0, 2)).reshape(length, HEAD)
    log_sum = jnp.transpose(log_sum.reshape(dilation, length // dilation)).reshape(length)
    return result, log_sum


def reference(queries, keys, values, w_out):
    length = queries.shape[1]
    positions = jnp.arange(length, dtype=jnp.int32).astype(jnp.float32)
    inverse = ROPE_BASE ** (-jnp.arange(0, HEAD, 2, dtype=jnp.float32) / HEAD)
    angles = positions[:, None] * inverse[None, :]
    cosine = jnp.cos(angles)[:, None, :]
    sine_part = jnp.sin(angles)[:, None, :]
    group_strides = (FIRST_STRIDE, SECOND_STRIDE, THIRD_STRIDE)
    results = []
    log_sums = []
    for group_id in range(len(group_strides)):
        query_f = queries[group_id].astype(jnp.float32).reshape(length, HEADS, HEAD)
        key_f = keys[group_id].astype(jnp.float32).reshape(length, HEADS, HEAD)
        turned_q = (turn_halves(query_f, cosine, sine_part) * HEAD ** -0.5).astype(jnp.bfloat16)
        turned_k = turn_halves(key_f, cosine, sine_part).astype(jnp.bfloat16)
        value_h = values[group_id].reshape(length, HEADS, HEAD)
        result, log_sum = lax.map(partial(strided_head, dilation=group_strides[group_id]),
                                  (jnp.transpose(turned_q, (1, 0, 2)),
                                   jnp.transpose(turned_k, (1, 0, 2)),
                                   jnp.transpose(value_h, (1, 0, 2))))
        results.append(jnp.transpose(result, (1, 0, 2)))
        log_sums.append(jnp.transpose(log_sum))
    shares = jax.nn.softmax(jnp.stack(log_sums), axis=0)
    attended = jnp.sum(shares[..., None] * jnp.stack(results), axis=0)
    attended = attended.astype(jnp.bfloat16).reshape(length, HEADS * HEAD)
    return jnp.dot(attended, w_out, preferred_element_type=jnp.float32).astype(jnp.bfloat16)
```

```python
import functools

import jax
import jax.numpy as jnp
import numpy as np
from jax import lax
from jax.experimental import pallas as pl
from jax.experimental.pallas import tpu as pltpu
from jax.sharding import PartitionSpec as P

HEAD = 128
KEYS = 128
STRIDES = (1, 4, 16)
ROPE_BASE = 10000.0
MASKED = -1e30
TEAM = 4

MESH = pl.DeviceIdType.MESH
F32 = jnp.float32
BF16 = jnp.bfloat16
Q, K, V = 0, 1, 2


def kernel(
    cfg,
    q_in, k_in, v_in, w_in, rows_in, base_in,
    o_ref,
    raw, ready, w_buf, rows_buf, base_buf, tables, perms,
    q_buf, q_next, kv0, kv1, kv2, acc, lse, acc1, lse1, bias,
    part_out, stat_out, part_in, stat_in, att, att_stat, back, back_stat, full, total_buf,
    in_sem, w_sem, t_sem, deal_send, deal_recv, first_send, first_recv, near_send, near_recv,
    turn_send, turn_recv, edge_send, edge_recv, part_send, part_recv, stat_send, stat_recv,
    ret_send, ret_recv, mark_send, mark_recv, d2d_send, d2d_recv,
):
    tokens, n_sp, heads = cfg
    width = heads * HEAD
    mine = heads // TEAM
    part = mine * HEAD
    span = TEAM * tokens
    few = tokens // STRIDES[2]
    lot = TEAM * few
    chunks = tokens // KEYS
    sp = lax.axis_index("sp")
    tp = lax.axis_index("tp")
    team = sp // TEAM
    me = lax.rem(sp, TEAM)
    has_next = sp + TEAM < n_sp
    has_prev = sp >= TEAM
    has_prev2 = sp >= 2 * TEAM
    middle = has_prev & has_next
    edge_next = sp + 1 < n_sp
    edge_prev = sp >= 1

    def partner(d):
        if d == 0:
            return me
        if d == 1:
            return me + 1 - 2 * lax.rem(me, 2)
        if d == 2:
            return lax.rem(me + 2, TEAM)
        return TEAM - 1 - me

    def cols(head):
        return slice(head * HEAD, (head + 1) * HEAD)

    def lanes_of(j):
        return pl.ds(pl.multiple_of(j * part, part), part)

    inputs = (q_in, k_in, v_in)
    loads = {}

    def load(kind, g):
        if (kind, g) == (V, 0):
            target = kv0.at[1, pl.ds(KEYS, tokens)]
        else:
            target = raw.at[kind, g]
        copy = pltpu.make_async_copy(inputs[kind].at[g], target, in_sem.at[kind, g])
        copy.start()
        loads[kind, g] = copy

    load(V, 2)
    rows_copy = pltpu.make_async_copy(rows_in, rows_buf, t_sem.at[0])
    rows_copy.start()
    base_copy = pltpu.make_async_copy(base_in, base_buf, t_sem.at[1])
    base_copy.start()
    for kind, g in ((K, 2), (Q, 2), (V, 1), (K, 1), (V, 0), (K, 0), (Q, 1), (Q, 0)):
        load(kind, g)
    w_loads = []
    for half in range(2):
        for head in range(mine):
            for s in range(TEAM):
                rows = pl.ds(half * width + s * part + head * HEAD, HEAD)
                copy = pltpu.make_async_copy(
                    w_in.at[rows],
                    w_buf.at[half, head, pl.ds(s * HEAD, HEAD)],
                    w_sem.at[half, head, s],
                )
                copy.start()
                w_loads.append(copy)

    barrier = pltpu.get_barrier_semaphore()

    def greet(where, when=None):
        def signal():
            pl.semaphore_signal(barrier, inc=1, device_id=where, device_id_type=MESH)

        if when is None:
            signal()
        else:
            pl.when(when)(signal)

    for d in range(1, TEAM):
        greet({"sp": team * TEAM + partner(d)})
    greet({"tp": 1 - tp})
    far_next = edge_next & (me == TEAM - 1)
    far_prev = edge_prev & (me == 0)
    greet({"sp": sp + TEAM}, has_next)
    greet({"sp": sp - TEAM}, has_prev)
    greet({"sp": sp + 1}, far_next)
    greet({"sp": sp - 1}, far_prev)

    row = lax.broadcasted_iota(jnp.int32, (tokens, tokens), 0)
    col = lax.broadcasted_iota(jnp.int32, (tokens, tokens), 1)

    def sorter(g):
        each = tokens // STRIDES[g]
        origin = lax.rem(row, each) * STRIDES[g] + row // each
        perms[g - 1] = jnp.where(origin == col, 1.0, 0.0).astype(BF16)

    def make_tables(g):
        c0, s0 = base_buf[sp, 0:1, :], base_buf[sp, 1:2, :]
        c, s = rows_buf[0, g], rows_buf[1, g]
        tables[0, g] = c0 * c - s0 * s
        tables[1, g] = s0 * c + c0 * s

    def turned(x, kind, g):
        x = x * tables[0, g] + pltpu.roll(x, HEAD // 2, 1) * tables[1, g]
        return x * HEAD ** (-0.5) if kind == Q else x

    def slot(kind, g, s):
        if kind == Q:
            return q_buf.at[g - 1, s]
        if g == 2:
            return kv2.at[kind - 1, TEAM + s]
        return kv1.at[kind - 1, 2 + s]

    def prepare(kind, g, d):
        j = partner(d)
        x = jnp.dot(perms[g - 1], raw[kind, g, :, lanes_of(j)], preferred_element_type=F32)
        for head in range(mine):
            y = x[:, cols(head)]
            if kind != V:
                y = turned(y, kind, g)
            if d == 0:
                slot(kind, g, me)[:, cols(head)] = y.astype(BF16)
            else:
                where = pl.ds(pl.multiple_of(j * part + head * HEAD, HEAD), HEAD)
                ready[kind, g - 1, :, where] = y.astype(BF16)

    def deal(kind, g, d):
        return pltpu.make_async_remote_copy(
            src_ref=ready.at[kind, g - 1, :, lanes_of(partner(d))],
            dst_ref=slot(kind, g, me),
            send_sem=deal_send.at[kind, g - 1, d],
            recv_sem=deal_recv.at[kind, g - 1, d],
            device_id={"sp": team * TEAM + partner(d)},
            device_id_type=MESH,
        )

    def wait_deal(kind, g, d):
        here = slot(kind, g, partner(d))
        pltpu.make_async_remote_copy(
            src_ref=here, dst_ref=here,
            send_sem=deal_send.at[kind, g - 1, d], recv_sem=deal_recv.at[kind, g - 1, d],
            device_id={"sp": team * TEAM + partner(d)}, device_id_type=MESH,
        ).wait_recv()

    def onward(src, dst, send, recv, to):
        return pltpu.make_async_remote_copy(
            src_ref=src, dst_ref=dst, send_sem=send, recv_sem=recv,
            device_id={"sp": lax.rem(to + n_sp, n_sp)}, device_id_type=MESH,
        )

    def first_hop(kind, s):
        return onward(
            kv2.at[kind - 1, TEAM + s], kv2.at[kind - 1, s],
            first_send.at[kind - 1, s], first_recv.at[kind - 1, s], sp + TEAM,
        )

    def near_hop(kind, i):
        return onward(
            kv1.at[kind - 1, TEAM + i], kv1.at[kind - 1, i],
            near_send.at[kind - 1, i], near_recv.at[kind - 1, i], sp + TEAM,
        )

    def turn_hop(s):
        return onward(q_buf.at[1, s], q_next.at[s], turn_send.at[s], turn_recv.at[s], sp - TEAM)

    def edge_hop(kind):
        return onward(
            kv0.at[kind - 1, pl.ds(tokens, KEYS)], kv0.at[kind - 1, pl.ds(0, KEYS)],
            edge_send.at[kind - 1], edge_recv.at[kind - 1], sp + 1,
        )

    def part_hop(head, j):
        rows = pl.ds(j * tokens, tokens)
        return onward(
            part_out.at[head, rows], part_in.at[head, rows],
            part_send.at[head, j], part_recv.at[head, j], sp + TEAM,
        )

    def stat_hop(head):
        return onward(
            stat_out.at[head], stat_in.at[head], stat_send.at[head], stat_recv.at[head], sp + TEAM,
        )

    def forward(kind, g, s):
        if kind == Q:
            if g == 2:
                pl.when(has_prev2)(lambda: turn_hop(s).start())
        elif g == 2:
            pl.when(has_next)(lambda: first_hop(kind, s).start())
        else:
            pl.when(has_next & (s >= TEAM - 2))(lambda: near_hop(kind, s - (TEAM - 2)).start())

    def arrive(kind, g, d):
        wait_deal(kind, g, d)
        forward(kind, g, partner(d))

    def send_all(kind, g, first=False):
        loads[kind, g].wait()
        for d in (3, 1, 2):
            prepare(kind, g, d)
            if first and d == 3:
                count = TEAM
                for extra in (has_next, has_prev, far_next, far_prev):
                    count = count + extra.astype(jnp.int32)
                pl.semaphore_wait(barrier, count)
            deal(kind, g, d).start()
        prepare(kind, g, 0)
        forward(kind, g, me)

    def own(kind):
        loads[kind, 0].wait()

        def step(h, carry):
            lanes = pl.ds(pl.multiple_of(h * HEAD, HEAD), HEAD)
            x = turned(raw[kind, 0, :, lanes].astype(F32), kind, 0).astype(BF16)
            if kind == K:
                kv0[0, KEYS:, lanes] = x
            else:
                ready[Q, 2, :, lanes] = x
            return carry

        lax.fori_loop(0, heads, step, 0, unroll=2)

    sorter(2)
    send_all(V, 2, first=True)
    rows_copy.wait()
    base_copy.wait()
    make_tables(2)
    send_all(K, 2)
    send_all(Q, 2)
    sorter(1)
    send_all(V, 1)
    for d in (1, 2, 3):
        arrive(V, 2, d)
    make_tables(1)
    send_all(K, 1)
    loads[V, 0].wait()
    pl.when(edge_next)(lambda: edge_hop(V).start())
    make_tables(0)
    own(K)
    pl.when(edge_next)(lambda: edge_hop(K).start())
    send_all(Q, 1)
    for d in (1, 2, 3):
        arrive(K, 2, d)
    own(Q)

    @pl.when(jnp.logical_not(edge_prev))
    def _():
        for kind in range(2):
            kv0[kind, 0:KEYS, :] = jnp.zeros((KEYS, width), BF16)

    @pl.when(jnp.logical_not(has_prev))
    def _():
        for kind in range(2):
            for s in range(2):
                kv1[kind, s] = jnp.zeros((tokens, part), BF16)
            for s in range(TEAM):
                kv2[kind, s] = jnp.zeros((tokens, part), BF16)

    @pl.when(jnp.logical_not(has_prev2))
    def _():
        for head in range(mine):
            part_in[head] = jnp.zeros((span, HEAD), BF16)
            stat_in[head] = jnp.full(stat_in.shape[1:], MASKED, F32)

    def band(index):
        a = lax.broadcasted_iota(jnp.int32, (KEYS, 2 * KEYS), 0)
        b = lax.broadcasted_iota(jnp.int32, (KEYS, 2 * KEYS), 1)
        allowed = (b >= jnp.maximum(a, KEYS - index)) & (b <= a + KEYS)
        return jnp.where(allowed, 0.0, MASKED)

    bias[0] = band(sp * tokens)
    bias[1] = band(KEYS)
    bias[2] = band(team * span)
    a = lax.broadcasted_iota(jnp.int32, (lot, 2 * lot), 0)
    b = lax.broadcasted_iota(jnp.int32, (lot, 2 * lot), 1)
    start = jnp.where(has_prev, 0, lot)
    bias[3, 0:lot, 0 : 2 * lot] = jnp.where((b <= a + lot) & (b >= start), 0.0, MASKED)
    bias[3, lot : 2 * lot, 0 : 2 * lot] = jnp.where(b >= a, 0.0, MASKED)

    def attend(tiles):
        scores = [
            lax.dot_general(t[0], t[1], (((1,), (1,)), ((), ())), preferred_element_type=F32)
            + t[3]
            for t in tiles
        ]
        best = [jnp.max(x, axis=1, keepdims=True) for x in scores]
        weights = [jnp.exp(x - m) for x, m in zip(scores, best)]
        outs = [
            jnp.dot(p.astype(BF16), t[2], preferred_element_type=F32)
            for p, t in zip(weights, tiles)
        ]
        total = [jnp.sum(p, axis=1, keepdims=True) for p in weights]
        for t, out, m, l in zip(tiles, outs, best, total):
            out_ref, log_ref, index, where = t[4]
            out_ref[(*index, where)] = out / l
            log_ref[(*index, where)] = jnp.broadcast_to(m + jnp.log(l), out.shape)

    def group1(n):
        def step(i, carry):
            tiles = []
            for u in range(mine):
                h = i * mine + u
                lanes = pl.ds(pl.multiple_of(h * HEAD, HEAD), HEAD)
                rows = slice(n * KEYS, (n + 2) * KEYS)
                tiles.append((
                    ready[Q, 2, n * KEYS : (n + 1) * KEYS, lanes],
                    kv0[0, rows, lanes], kv0[1, rows, lanes], bias[min(n, 1)],
                    (acc1, lse1, (h,), pl.ds(n * KEYS, KEYS)),
                ))
            attend(tiles)
            return carry

        lax.fori_loop(0, heads // mine, step, 0, unroll=2)

    def group2():
        each = tokens // STRIDES[1]
        pair = KEYS // each

        def step(n, carry):
            r, i = n // (TEAM // pair), lax.rem(n, TEAM // pair)
            rows = pl.ds(pl.multiple_of(r * each, each), each)
            tiles = []
            for head in range(mine):
                query = q_buf[0, pl.ds(i * pair, pair), rows, cols(head)].reshape(KEYS, HEAD)
                key = kv1[0, pl.ds(i * pair, 2 * pair), rows, cols(head)].reshape(2 * KEYS, HEAD)
                value = kv1[1, pl.ds(i * pair, 2 * pair), rows, cols(head)].reshape(2 * KEYS, HEAD)
                where = pl.ds(r + STRIDES[1] * KEYS * i, KEYS, stride=STRIDES[1])
                tiles.append((
                    query, key, value, bias[2 - jnp.minimum(i, 1)], (acc, lse, (0, head), where),
                ))
            attend(tiles)
            return carry

        lax.fori_loop(0, STRIDES[1] * (TEAM // pair), step, 0, unroll=2)

    def group3(head, queries, count, off, which):
        for first in range(0, STRIDES[2], 4):
            tiles = []
            for r in range(first, first + 4):
                rows = slice(r * few, (r + 1) * few)
                query = queries(rows).reshape(lot, HEAD)
                key = kv2[0, 0:count, rows, cols(head)].reshape(count * few, HEAD)
                value = kv2[1, 0:count, rows, cols(head)].reshape(count * few, HEAD)
                where = pl.ds(r, lot, stride=STRIDES[2])
                tiles.append((query, key, value, off, (acc, lse, (which, head), where)))
            attend(tiles)

    eye = (
        lax.broadcasted_iota(jnp.int32, (KEYS, KEYS), 0)
        == lax.broadcasted_iota(jnp.int32, (KEYS, KEYS), 1)
    )

    def to_row(x):
        return jnp.sum(jnp.where(eye, x, 0.0), axis=0, keepdims=True)

    def to_col(x):
        return jnp.sum(jnp.where(eye, x, 0.0), axis=1, keepdims=True)

    for d in (1, 2, 3):
        arrive(Q, 2, d)
    group1(1)
    for d in (1, 2, 3):
        arrive(V, 1, d)

    @pl.when(has_prev)
    def _():
        for s in range(TEAM):
            for kind in (V, K):
                first_hop(kind, s).wait_recv()

    @pl.when(middle)
    def _():
        for s in range(TEAM):
            turn_hop(s).wait_recv()
        off = bias[3, lot : 2 * lot, 0:lot]
        for head in range(mine):
            group3(head, lambda rows: q_next[:, rows, cols(head)], TEAM, off, 2)
            for j in range(TEAM):
                for c in range(j * chunks, (j + 1) * chunks):
                    rows = slice(c * KEYS, (c + 1) * KEYS)
                    part_out[head, rows] = acc[2, head, rows, :].astype(BF16)
                    stat_out[head, c : c + 1, :] = to_row(lse[2, head, rows, :])
                part_hop(head, j).start()
            stat_hop(head).start()

    for d in (1, 2, 3):
        arrive(K, 1, d)
    for head in range(mine):
        off = bias[3, 0:lot, 0 : 2 * lot]
        group3(head, lambda rows: q_buf[1, :, rows, cols(head)], 2 * TEAM, off, 1)

    @pl.when(edge_prev)
    def _():
        for kind in (V, K):
            edge_hop(kind).wait_recv()

    group1(0)
    for d in (1, 2, 3):
        wait_deal(Q, 1, d)

    @pl.when(has_prev)
    def _():
        for kind in (V, K):
            for i in range(2):
                near_hop(kind, i).wait_recv()

    group2()

    def merge(j, head, out_ref, log_ref):
        for c in range(chunks):
            rows = pl.ds(pl.multiple_of(j * tokens + c * KEYS, KEYS), KEYS)
            logs = [lse[g, head, rows, :] for g in range(2)]
            logs.append(to_col(stat_in[head, pl.ds(j * chunks + c, 1), :]))
            outs = [acc[g, head, rows, :] for g in range(2)]
            outs.append(part_in[head, rows, :].astype(F32))
            peak = jnp.maximum(jnp.maximum(logs[0], logs[1]), logs[2])
            scales = [jnp.exp(x - peak) for x in logs]
            lower = scales[0] + scales[1] + scales[2]
            upper = scales[0] * outs[0] + scales[1] * outs[1] + scales[2] * outs[2]
            out_ref[c * KEYS : (c + 1) * KEYS, :] = (upper / lower).astype(BF16)
            log_ref[c : c + 1, :] = to_row(peak + jnp.log(lower))

    def place_of(s):
        return pl.ds(pl.multiple_of(s * HEAD, HEAD), HEAD)

    def home(d, head):
        peer = partner(d)
        where = {"sp": team * TEAM + peer}
        return (
            pltpu.make_async_remote_copy(
                src_ref=att.at[head, peer], dst_ref=back.at[head, me],
                send_sem=ret_send.at[d, head], recv_sem=ret_recv.at[d, head],
                device_id=where, device_id_type=MESH,
            ),
            pltpu.make_async_remote_copy(
                src_ref=att_stat.at[head, peer], dst_ref=back_stat.at[head, me],
                send_sem=mark_send.at[d, head], recv_sem=mark_recv.at[d, head],
                device_id=where, device_id_type=MESH,
            ),
        )

    def wait_home(d, head):
        peer = partner(d)
        for ref, send, recv in (
            (back, ret_send, ret_recv), (back_stat, mark_send, mark_recv),
        ):
            here = ref.at[head, peer]
            pltpu.make_async_remote_copy(
                src_ref=here, dst_ref=here, send_sem=send.at[d, head], recv_sem=recv.at[d, head],
                device_id={"sp": team * TEAM + peer}, device_id_type=MESH,
            ).wait_recv()

    def finish(d, head):
        s = partner(d)
        h = s * mine + head
        for c in range(chunks):
            rows = slice(c * KEYS, (c + 1) * KEYS)
            log_a = lse1[h, rows, :]
            log_b = to_col(back_stat[head, s, c : c + 1, :])
            peak = jnp.maximum(log_a, log_b)
            scale_a, scale_b = jnp.exp(log_a - peak), jnp.exp(log_b - peak)
            upper = scale_a * acc1[h, rows, :] + scale_b * back[head, s, rows, :].astype(F32)
            full[tp, head, rows, place_of(s)] = (upper / (scale_a + scale_b)).astype(BF16)

    def twin(d, half, head):
        here = full.at[half, head, :, place_of(partner(d))]
        return pltpu.make_async_remote_copy(
            src_ref=here, dst_ref=here,
            send_sem=d2d_send.at[d, head], recv_sem=d2d_recv.at[d, head],
            device_id={"tp": 1 - tp}, device_id_type=MESH,
        )

    for copy in w_loads:
        copy.wait()
    for head in range(mine):

        @pl.when(has_prev2)
        def _():
            stat_hop(head).wait_recv()
            for j in range(TEAM):
                part_hop(head, j).wait_recv()

        for d in (3, 1, 2, 0):
            j = partner(d)
            if d:
                merge(j, head, att.at[head, j], att_stat.at[head, j])
                for copy in home(d, head):
                    copy.start()
            else:
                merge(j, head, back.at[head, j], back_stat.at[head, j])
        finish(0, head)
        twin(0, tp, head).start()
    for head in range(mine):
        for d in (1, 2, 3):
            wait_home(d, head)
            finish(d, head)
            twin(d, tp, head).start()
        product = jnp.dot(full[tp, head], w_buf[tp, head], preferred_element_type=F32)
        for d in range(TEAM):
            twin(d, 1 - tp, head).wait_recv()
        product = product + jnp.dot(
            full[1 - tp, head], w_buf[1 - tp, head], preferred_element_type=F32
        )
        if head == 0:
            total_buf[...] = product
        elif head < mine - 1:
            total_buf[...] += product
        else:
            o_ref[...] = (total_buf[...] + product).astype(BF16)

    for kind in range(3):
        for g in (1, 2):
            for d in range(1, TEAM):
                deal(kind, g, d).wait_send()
    for head in range(mine):
        for d in range(1, TEAM):
            for copy in home(d, head):
                copy.wait_send()
        for d in range(TEAM):
            twin(d, tp, head).wait_send()

    @pl.when(has_next)
    def _():
        for kind in (V, K):
            for s in range(TEAM):
                first_hop(kind, s).wait_send()
            for i in range(2):
                near_hop(kind, i).wait_send()

    @pl.when(edge_next)
    def _():
        for kind in (V, K):
            edge_hop(kind).wait_send()

    @pl.when(has_prev2)
    def _():
        for s in range(TEAM):
            turn_hop(s).wait_send()

    @pl.when(middle)
    def _():
        for head in range(mine):
            for j in range(TEAM):
                part_hop(head, j).wait_send()
            stat_hop(head).wait_send()


def angle_tables(tokens, n_sp):
    inverse = ROPE_BASE ** (-np.arange(0, HEAD, 2) / HEAD)

    def pair(positions):
        angles = positions[:, None] * inverse[None, :]
        cosine, sine = np.cos(angles), np.sin(angles)
        return (
            np.concatenate([cosine, cosine], axis=1),
            np.concatenate([-sine, sine], axis=1),
        )

    by_group = []
    for stride in STRIDES:
        order = np.arange(tokens).reshape(tokens // stride, stride).T.reshape(-1)
        by_group.append(pair(order.astype(np.float64)))
    rows = np.stack([np.stack([t[i] for t in by_group]) for i in range(2)])
    base = np.zeros((n_sp, 8, HEAD))
    base[:, 0], base[:, 1] = pair(np.arange(n_sp) * float(tokens))
    return rows.astype(np.float32), base.astype(np.float32)


def shards(n_sp, queries, keys, values, w_out):
    tokens, width = queries.shape[1:]
    heads = width // HEAD
    mine = heads // TEAM
    part = mine * HEAD
    span = TEAM * tokens
    rows, base = angle_tables(tokens, n_sp)
    any_spec = pl.BlockSpec(memory_space=pl.ANY)
    vmem = pl.BlockSpec(memory_space=pltpu.VMEM)
    dma = pltpu.SemaphoreType.DMA
    return pl.pallas_call(
        functools.partial(kernel, (tokens, n_sp, heads)),
        out_shape=jax.ShapeDtypeStruct((tokens, w_out.shape[1]), BF16),
        in_specs=[any_spec] * 6,
        out_specs=vmem,
        scratch_shapes=[
            pltpu.VMEM((3, 3, tokens, width), BF16),
            pltpu.VMEM((3, 3, tokens, width), BF16),
            pltpu.VMEM((2, mine, TEAM * HEAD, w_out.shape[1]), BF16),
            pltpu.VMEM(rows.shape, F32),
            pltpu.VMEM(base.shape, F32),
            pltpu.VMEM(rows.shape, F32),
            pltpu.VMEM((2, tokens, tokens), BF16),
            pltpu.VMEM((2, TEAM, tokens, part), BF16),
            pltpu.VMEM((TEAM, tokens, part), BF16),
            pltpu.VMEM((2, KEYS + tokens, width), BF16),
            pltpu.VMEM((2, 2 + TEAM, tokens, part), BF16),
            pltpu.VMEM((2, 2 * TEAM, tokens, part), BF16),
            pltpu.VMEM((3, mine, span, HEAD), F32),
            pltpu.VMEM((3, mine, span, HEAD), F32),
            pltpu.VMEM((heads, tokens, HEAD), F32),
            pltpu.VMEM((heads, tokens, HEAD), F32),
            pltpu.VMEM((4, KEYS, 2 * KEYS), F32),
            pltpu.VMEM((mine, span, HEAD), BF16),
            pltpu.VMEM((mine, span // KEYS, KEYS), F32),
            pltpu.VMEM((mine, span, HEAD), BF16),
            pltpu.VMEM((mine, span // KEYS, KEYS), F32),
            pltpu.VMEM((mine, TEAM, tokens, HEAD), BF16),
            pltpu.VMEM((mine, TEAM, 8, KEYS), F32),
            pltpu.VMEM((mine, TEAM, tokens, HEAD), BF16),
            pltpu.VMEM((mine, TEAM, 8, KEYS), F32),
            pltpu.VMEM((2, mine, tokens, TEAM * HEAD), BF16),
            pltpu.VMEM((tokens, w_out.shape[1]), F32),
            dma((3, 3)),
            dma((2, mine, TEAM)),
            dma((2,)),
            dma((3, 2, TEAM)),
            dma((3, 2, TEAM)),
            dma((2, TEAM)),
            dma((2, TEAM)),
            dma((2, 2)),
            dma((2, 2)),
            dma((TEAM,)),
            dma((TEAM,)),
            dma((2,)),
            dma((2,)),
            dma((mine, TEAM)),
            dma((mine, TEAM)),
            dma((mine,)),
            dma((mine,)),
            dma((TEAM, mine)),
            dma((TEAM, mine)),
            dma((TEAM, mine)),
            dma((TEAM, mine)),
            dma((TEAM, mine)),
            dma((TEAM, mine)),
        ],
        compiler_params=pltpu.CompilerParams(
            collective_id=0, has_side_effects=True, vmem_limit_bytes=60 * 1024 * 1024
        ),
    )(queries, keys, values, w_out, jnp.asarray(rows), jnp.asarray(base))


def solution(mesh):
    return jax.shard_map(
        functools.partial(shards, mesh.shape["sp"]),
        mesh=mesh,
        in_specs=(P(None, "sp", "tp"), P(None, "sp", "tp"), P(None, "sp", "tp"), P(None, "tp")),
        out_specs=P("sp", "tp"),
        check_vma=False,
    )
```

```python
import functools

import jax
import jax.numpy as jnp
import numpy as np
from jax import lax
from jax.experimental import pallas as pl
from jax.experimental.pallas import tpu as pltpu
from jax.sharding import PartitionSpec as P

HEAD = 128
KEYS = 128
STRIDES = (1, 4, 16)
ROPE_BASE = 10000.0
MASKED = -1e30
TEAM = 4

MESH = pl.DeviceIdType.MESH
F32 = jnp.float32
BF16 = jnp.bfloat16
Q, K, V = 0, 1, 2


def kernel(
    cfg,
    q_in, k_in, v_in, w_in, angles_in,
    o_ref,
    raw, ready, w_buf, angles, tables, perms,
    q_buf, q_next, kv0, kv1, kv2, relay, acc, lse, acc1, lse1, bias,
    part_out, stat_out, part_in, stat_in, att, att_stat, back, back_stat, full, total_buf,
    in_sem, w_sem, t_sem, deal_send, deal_recv, first_send, first_recv, near_send, near_recv,
    turn_send, turn_recv, edge_send, edge_recv, relay_send, relay_recv, part_send, part_recv, stat_send, stat_recv,
    ret_send, ret_recv, mark_send, mark_recv, d2d_send, d2d_recv,
):
    tokens, n_sp, heads = cfg
    width = heads * HEAD
    mine = heads // TEAM
    part = mine * HEAD
    span = TEAM * tokens
    few = tokens // STRIDES[2]
    lot = TEAM * few
    chunks = tokens // KEYS
    sp = lax.axis_index("sp")
    tp = lax.axis_index("tp")
    team = sp // TEAM
    me = lax.rem(sp, TEAM)
    has_next = sp + TEAM < n_sp
    has_prev = sp >= TEAM
    has_prev2 = sp >= 2 * TEAM
    middle = has_prev & has_next
    edge_next = sp + 1 < n_sp
    edge_prev = sp >= 1
    relay_next = (me == TEAM - 2) & (sp + 2 < n_sp)
    relay_prev = (me == 0) & (sp >= 2)

    def partner(d):
        if d == 0:
            return me
        if d == 1:
            return me + 1 - 2 * lax.rem(me, 2)
        if d == 2:
            return lax.rem(me + 2, TEAM)
        return TEAM - 1 - me

    def cols(head):
        return slice(head * HEAD, (head + 1) * HEAD)

    def lanes_of(j):
        return pl.ds(pl.multiple_of(j * part, part), part)

    inputs = (q_in, k_in, v_in)
    loads = {}

    def load(kind, g):
        if (kind, g) == (V, 0):
            target = kv0.at[1, pl.ds(KEYS, tokens)]
        else:
            target = raw.at[kind, g]
        copy = pltpu.make_async_copy(inputs[kind].at[g], target, in_sem.at[kind, g])
        copy.start()
        loads[kind, g] = copy

    load(V, 2)
    angles_copy = pltpu.make_async_copy(angles_in, angles, t_sem)
    angles_copy.start()
    for kind, g in ((K, 2), (Q, 2), (V, 1), (K, 1), (V, 0), (K, 0), (Q, 1), (Q, 0)):
        load(kind, g)
    barrier = pltpu.get_barrier_semaphore()

    def greet(where, when=None):
        def signal():
            pl.semaphore_signal(barrier, inc=1, device_id=where, device_id_type=MESH)

        if when is None:
            signal()
        else:
            pl.when(when)(signal)

    for d in range(1, TEAM):
        greet({"sp": team * TEAM + partner(d)})
    greet({"tp": 1 - tp})
    far_next = edge_next & (me == TEAM - 1)
    far_prev = edge_prev & (me == 0)
    greet({"sp": sp + TEAM}, has_next)
    greet({"sp": sp - TEAM}, has_prev)
    greet({"sp": sp + 1}, far_next)
    greet({"sp": sp - 1}, far_prev)
    greet({"sp": sp + 2}, relay_next)
    greet({"sp": sp - 2}, relay_prev)

    row = lax.broadcasted_iota(jnp.int32, (tokens, tokens), 0)
    col = lax.broadcasted_iota(jnp.int32, (tokens, tokens), 1)

    def sorter(g):
        each = tokens // STRIDES[g]
        origin = lax.rem(row, each) * STRIDES[g] + row // each
        perms[g - 1] = jnp.where(origin == col, 1.0, 0.0).astype(BF16)

    def make_tables(g):
        at = pl.multiple_of(6 * tokens + 8 * sp, 8)
        base = angles[pl.ds(at, 8), :]
        c0, s0 = base[0:1, :], base[1:2, :]
        c = angles[g * tokens : (g + 1) * tokens, :]
        s = angles[(3 + g) * tokens : (4 + g) * tokens, :]
        tables[0, g] = c0 * c - s0 * s
        tables[1, g] = s0 * c + c0 * s

    def turned(x, kind, g):
        x = x * tables[0, g] + pltpu.roll(x, HEAD // 2, 1) * tables[1, g]
        return x * HEAD ** (-0.5) if kind == Q else x

    def slot(kind, g, s):
        if kind == Q:
            return q_buf.at[g - 1, s]
        if g == 2:
            return kv2.at[kind - 1, TEAM + s]
        return kv1.at[kind - 1, 2 + s]

    def prepare(kind, g, d):
        j = partner(d)
        x = jnp.dot(perms[g - 1], raw[kind, g, :, lanes_of(j)], preferred_element_type=F32)
        for head in range(mine):
            y = x[:, cols(head)]
            if kind != V:
                y = turned(y, kind, g)
            if d == 0:
                slot(kind, g, me)[:, cols(head)] = y.astype(BF16)
            else:
                where = pl.ds(pl.multiple_of(j * part + head * HEAD, HEAD), HEAD)
                ready[kind, g - 1, :, where] = y.astype(BF16)

    def deal(kind, g, d):
        return pltpu.make_async_remote_copy(
            src_ref=ready.at[kind, g - 1, :, lanes_of(partner(d))],
            dst_ref=slot(kind, g, me),
            send_sem=deal_send.at[kind, g - 1, d],
            recv_sem=deal_recv.at[kind, g - 1, d],
            device_id={"sp": team * TEAM + partner(d)},
            device_id_type=MESH,
        )

    def wait_deal(kind, g, d):
        here = slot(kind, g, partner(d))
        pltpu.make_async_remote_copy(
            src_ref=here, dst_ref=here,
            send_sem=deal_send.at[kind, g - 1, d], recv_sem=deal_recv.at[kind, g - 1, d],
            device_id={"sp": team * TEAM + partner(d)}, device_id_type=MESH,
        ).wait_recv()

    def onward(src, dst, send, recv, to):
        return pltpu.make_async_remote_copy(
            src_ref=src, dst_ref=dst, send_sem=send, recv_sem=recv,
            device_id={"sp": lax.rem(to + n_sp, n_sp)}, device_id_type=MESH,
        )

    def first_hop(kind, s):
        return onward(
            kv2.at[kind - 1, TEAM + s], kv2.at[kind - 1, s],
            first_send.at[kind - 1, s], first_recv.at[kind - 1, s], sp + TEAM,
        )

    def near_hop(kind, i):
        return onward(
            kv1.at[kind - 1, TEAM + i], kv1.at[kind - 1, i],
            near_send.at[kind - 1, i], near_recv.at[kind - 1, i], sp + TEAM,
        )

    def turn_hop(s):
        return onward(q_buf.at[1, s], q_next.at[s], turn_send.at[s], turn_recv.at[s], sp - TEAM)

    def edge_hop(kind):
        return onward(
            kv0.at[kind - 1, pl.ds(tokens, KEYS)], kv0.at[kind - 1, pl.ds(0, KEYS)],
            edge_send.at[kind - 1], edge_recv.at[kind - 1], sp + 1,
        )

    def relay_in():
        return onward(
            kv0.at[1, pl.ds(tokens, KEYS)], relay, relay_send.at[0], relay_recv, sp - 1,
        )

    def relay_out():
        return onward(
            relay, kv0.at[1, pl.ds(0, KEYS)], relay_send.at[1], edge_recv.at[1], sp + 2,
        )

    def part_hop(head, j):
        rows = pl.ds(j * tokens, tokens)
        return onward(
            part_out.at[head, rows], part_in.at[head, rows],
            part_send.at[head, j], part_recv.at[head, j], sp + TEAM,
        )

    def stat_hop(head):
        return onward(
            stat_out.at[head], stat_in.at[head], stat_send.at[head], stat_recv.at[head], sp + TEAM,
        )

    def forward(kind, g, s):
        if kind == Q:
            if g == 2:
                pl.when(has_prev2)(lambda: turn_hop(s).start())
        elif g == 2:
            pl.when(has_next)(lambda: first_hop(kind, s).start())
        else:
            pl.when(has_next & (s >= TEAM - 2))(lambda: near_hop(kind, s - (TEAM - 2)).start())

    def arrive(kind, g, d):
        wait_deal(kind, g, d)
        forward(kind, g, partner(d))

    def send_all(kind, g, first=False):
        loads[kind, g].wait()
        for d in (3, 1, 2):
            prepare(kind, g, d)
            if first and d == 3:
                count = TEAM
                for extra in (has_next, has_prev, far_next, far_prev, relay_next, relay_prev):
                    count = count + extra.astype(jnp.int32)
                pl.semaphore_wait(barrier, count)
            deal(kind, g, d).start()
        prepare(kind, g, 0)
        forward(kind, g, me)

    def own(kind):
        loads[kind, 0].wait()

        def step(h, carry):
            lanes = pl.ds(pl.multiple_of(h * HEAD, HEAD), HEAD)
            x = turned(raw[kind, 0, :, lanes].astype(F32), kind, 0).astype(BF16)
            if kind == K:
                kv0[0, KEYS:, lanes] = x
            else:
                ready[Q, 2, :, lanes] = x
            return carry

        lax.fori_loop(0, heads, step, 0, unroll=2)

    sorter(2)
    send_all(V, 2, first=True)
    w_loads = []
    for half in range(2):
        for head in range(mine):
            for s in range(TEAM):
                rows = pl.ds(half * width + s * part + head * HEAD, HEAD)
                copy = pltpu.make_async_copy(
                    w_in.at[rows],
                    w_buf.at[half, head, pl.ds(s * HEAD, HEAD)],
                    w_sem.at[half, head, s],
                )
                copy.start()
                w_loads.append(copy)
    angles_copy.wait()
    make_tables(2)
    send_all(K, 2)
    send_all(Q, 2)
    sorter(1)
    send_all(V, 1)
    for d in (1, 2, 3):
        arrive(V, 2, d)
    make_tables(1)
    send_all(K, 1)
    send_all(Q, 1)
    make_tables(0)
    own(K)
    loads[V, 0].wait()

    @pl.when(edge_next & (me < TEAM - 1))
    def _():
        for kind in (V, K):
            edge_hop(kind).start()

    @pl.when(far_next)
    def _():
        relay_in().start()

    own(Q)
    for d in (1, 2, 3):
        arrive(K, 2, d)

    @pl.when(jnp.logical_not(edge_prev))
    def _():
        for kind in range(2):
            kv0[kind, 0:KEYS, :] = jnp.zeros((KEYS, width), BF16)

    @pl.when(jnp.logical_not(has_prev))
    def _():
        for kind in range(2):
            for s in range(2):
                kv1[kind, s] = jnp.zeros((tokens, part), BF16)
            for s in range(TEAM):
                kv2[kind, s] = jnp.zeros((tokens, part), BF16)

    @pl.when(jnp.logical_not(has_prev2))
    def _():
        for head in range(mine):
            part_in[head] = jnp.zeros((span, HEAD), BF16)
            stat_in[head] = jnp.full(stat_in.shape[1:], MASKED, F32)

    def band(index):
        a = lax.broadcasted_iota(jnp.int32, (KEYS, 2 * KEYS), 0)
        b = lax.broadcasted_iota(jnp.int32, (KEYS, 2 * KEYS), 1)
        allowed = (b >= jnp.maximum(a, KEYS - index)) & (b <= a + KEYS)
        return jnp.where(allowed, 0.0, MASKED)

    bias[0] = band(sp * tokens)
    bias[1] = band(KEYS)
    bias[2] = band(team * span)
    a = lax.broadcasted_iota(jnp.int32, (lot, 2 * lot), 0)
    b = lax.broadcasted_iota(jnp.int32, (lot, 2 * lot), 1)
    start = jnp.where(has_prev, 0, lot)
    bias[3, 0:lot, 0 : 2 * lot] = jnp.where((b <= a + lot) & (b >= start), 0.0, MASKED)
    bias[3, lot : 2 * lot, 0 : 2 * lot] = jnp.where(b >= a, 0.0, MASKED)

    def attend(tiles):
        scores = [
            lax.dot_general(t[0], t[1], (((1,), (1,)), ((), ())), preferred_element_type=F32)
            + t[3]
            for t in tiles
        ]
        best = [jnp.max(x, axis=1, keepdims=True) for x in scores]
        weights = [jnp.exp(x - m) for x, m in zip(scores, best)]
        outs = [
            jnp.dot(p.astype(BF16), t[2], preferred_element_type=F32)
            for p, t in zip(weights, tiles)
        ]
        total = [jnp.sum(p, axis=1, keepdims=True) for p in weights]
        for t, out, m, l in zip(tiles, outs, best, total):
            out_ref, log_ref, index, where = t[4]
            out_ref[(*index, where)] = out / l
            log_ref[(*index, where)] = jnp.broadcast_to(m + jnp.log(l), out.shape)

    def group1(n):
        def step(i, carry):
            tiles = []
            for u in range(mine):
                h = i * mine + u
                lanes = pl.ds(pl.multiple_of(h * HEAD, HEAD), HEAD)
                rows = slice(n * KEYS, (n + 2) * KEYS)
                tiles.append((
                    ready[Q, 2, n * KEYS : (n + 1) * KEYS, lanes],
                    kv0[0, rows, lanes], kv0[1, rows, lanes], bias[min(n, 1)],
                    (acc1, lse1, (h,), pl.ds(n * KEYS, KEYS)),
                ))
            attend(tiles)
            return carry

        lax.fori_loop(0, heads // mine, step, 0, unroll=2)

    def group2():
        each = tokens // STRIDES[1]
        pair = KEYS // each

        def step(n, carry):
            r, i = n // (TEAM // pair), lax.rem(n, TEAM // pair)
            rows = pl.ds(pl.multiple_of(r * each, each), each)
            tiles = []
            for head in range(mine):
                query = q_buf[0, pl.ds(i * pair, pair), rows, cols(head)].reshape(KEYS, HEAD)
                key = kv1[0, pl.ds(i * pair, 2 * pair), rows, cols(head)].reshape(2 * KEYS, HEAD)
                value = kv1[1, pl.ds(i * pair, 2 * pair), rows, cols(head)].reshape(2 * KEYS, HEAD)
                where = pl.ds(r + STRIDES[1] * KEYS * i, KEYS, stride=STRIDES[1])
                tiles.append((
                    query, key, value, bias[2 - jnp.minimum(i, 1)], (acc, lse, (0, head), where),
                ))
            attend(tiles)
            return carry

        lax.fori_loop(0, STRIDES[1] * (TEAM // pair), step, 0, unroll=2)

    def group3(head, queries, count, off, which):
        for first in range(0, STRIDES[2], 4):
            tiles = []
            for r in range(first, first + 4):
                rows = slice(r * few, (r + 1) * few)
                query = queries(rows).reshape(lot, HEAD)
                key = kv2[0, 0:count, rows, cols(head)].reshape(count * few, HEAD)
                value = kv2[1, 0:count, rows, cols(head)].reshape(count * few, HEAD)
                where = pl.ds(r, lot, stride=STRIDES[2])
                tiles.append((query, key, value, off, (acc, lse, (which, head), where)))
            attend(tiles)

    eye = (
        lax.broadcasted_iota(jnp.int32, (KEYS, KEYS), 0)
        == lax.broadcasted_iota(jnp.int32, (KEYS, KEYS), 1)
    )

    def to_row(x):
        return jnp.sum(jnp.where(eye, x, 0.0), axis=0, keepdims=True)

    def to_col(x):
        return jnp.sum(jnp.where(eye, x, 0.0), axis=1, keepdims=True)

    group1(1)
    for d in (1, 2, 3):
        arrive(Q, 2, d)
    for d in (1, 2, 3):
        arrive(V, 1, d)

    @pl.when(has_prev)
    def _():
        for s in range(TEAM):
            for kind in (V, K):
                first_hop(kind, s).wait_recv()

    def pass_on(head):
        @pl.when(middle)
        def _():
            if head == 0:
                for s in range(TEAM):
                    turn_hop(s).wait_recv()
            off = bias[3, lot : 2 * lot, 0:lot]
            group3(head, lambda rows: q_next[:, rows, cols(head)], TEAM, off, 2)
            for j in range(TEAM):
                for c in range(j * chunks, (j + 1) * chunks):
                    rows = slice(c * KEYS, (c + 1) * KEYS)
                    part_out[head, rows] = acc[2, head, rows, :].astype(BF16)
                    stat_out[head, c : c + 1, :] = to_row(lse[2, head, rows, :])
                part_hop(head, j).start()
            stat_hop(head).start()

    pass_on(0)
    for d in (1, 2, 3):
        arrive(K, 1, d)
    for head in range(1, mine):
        pass_on(head)

    @pl.when(far_next)
    def _():
        edge_hop(K).start()

    for head in range(mine):
        off = bias[3, 0:lot, 0 : 2 * lot]
        group3(head, lambda rows: q_buf[1, :, rows, cols(head)], 2 * TEAM, off, 1)
    for d in (1, 2, 3):
        wait_deal(Q, 1, d)

    @pl.when(relay_next)
    def _():
        onward(relay, relay, relay_send.at[0], relay_recv, sp + 1).wait_recv()
        relay_out().start()

    @pl.when(has_prev)
    def _():
        for kind in (V, K):
            for i in range(2):
                near_hop(kind, i).wait_recv()

    group2()

    def merge(j, head, out_ref, log_ref):
        for c in range(chunks):
            rows = pl.ds(pl.multiple_of(j * tokens + c * KEYS, KEYS), KEYS)
            logs = [lse[g, head, rows, :] for g in range(2)]
            logs.append(to_col(stat_in[head, pl.ds(j * chunks + c, 1), :]))
            outs = [acc[g, head, rows, :] for g in range(2)]
            outs.append(part_in[head, rows, :].astype(F32))
            peak = jnp.maximum(jnp.maximum(logs[0], logs[1]), logs[2])
            scales = [jnp.exp(x - peak) for x in logs]
            lower = scales[0] + scales[1] + scales[2]
            upper = scales[0] * outs[0] + scales[1] * outs[1] + scales[2] * outs[2]
            out_ref[c * KEYS : (c + 1) * KEYS, :] = (upper / lower).astype(BF16)
            log_ref[c : c + 1, :] = to_row(peak + jnp.log(lower))

    def place_of(s):
        return pl.ds(pl.multiple_of(s * HEAD, HEAD), HEAD)

    def home(d, head):
        peer = partner(d)
        where = {"sp": team * TEAM + peer}
        return (
            pltpu.make_async_remote_copy(
                src_ref=att.at[head, peer], dst_ref=back.at[head, me],
                send_sem=ret_send.at[d, head], recv_sem=ret_recv.at[d, head],
                device_id=where, device_id_type=MESH,
            ),
            pltpu.make_async_remote_copy(
                src_ref=att_stat.at[head, peer], dst_ref=back_stat.at[head, me],
                send_sem=mark_send.at[d, head], recv_sem=mark_recv.at[d, head],
                device_id=where, device_id_type=MESH,
            ),
        )

    def wait_home(d, head):
        peer = partner(d)
        for ref, send, recv in (
            (back, ret_send, ret_recv), (back_stat, mark_send, mark_recv),
        ):
            here = ref.at[head, peer]
            pltpu.make_async_remote_copy(
                src_ref=here, dst_ref=here, send_sem=send.at[d, head], recv_sem=recv.at[d, head],
                device_id={"sp": team * TEAM + peer}, device_id_type=MESH,
            ).wait_recv()

    def finish(d, head):
        s = partner(d)
        h = s * mine + head
        for c in range(chunks):
            rows = slice(c * KEYS, (c + 1) * KEYS)
            log_a = lse1[h, rows, :]
            log_b = to_col(back_stat[head, s, c : c + 1, :])
            peak = jnp.maximum(log_a, log_b)
            scale_a, scale_b = jnp.exp(log_a - peak), jnp.exp(log_b - peak)
            upper = scale_a * acc1[h, rows, :] + scale_b * back[head, s, rows, :].astype(F32)
            full[tp, head, rows, place_of(s)] = (upper / (scale_a + scale_b)).astype(BF16)

    def twin(d, half, head):
        here = full.at[half, head, :, place_of(partner(d))]
        return pltpu.make_async_remote_copy(
            src_ref=here, dst_ref=here,
            send_sem=d2d_send.at[d, head], recv_sem=d2d_recv.at[d, head],
            device_id={"tp": 1 - tp}, device_id_type=MESH,
        )

    for copy in w_loads:
        copy.wait()
    for head in range(mine):

        @pl.when(has_prev2)
        def _():
            stat_hop(head).wait_recv()
            for j in range(TEAM):
                part_hop(head, j).wait_recv()

        for d in (3, 1, 2, 0):
            j = partner(d)
            if d:
                merge(j, head, att.at[head, j], att_stat.at[head, j])
                for copy in home(d, head):
                    copy.start()
            else:
                merge(j, head, back.at[head, j], back_stat.at[head, j])

    @pl.when(edge_prev)
    def _():
        for kind in (V, K):
            edge_hop(kind).wait_recv()

    group1(0)
    for head in range(mine):
        finish(0, head)
        twin(0, tp, head).start()
    for head in range(mine):
        for d in (1, 2, 3):
            wait_home(d, head)
            finish(d, head)
            twin(d, tp, head).start()
        product = jnp.dot(full[tp, head], w_buf[tp, head], preferred_element_type=F32)
        for d in range(TEAM):
            twin(d, 1 - tp, head).wait_recv()
        product = product + jnp.dot(
            full[1 - tp, head], w_buf[1 - tp, head], preferred_element_type=F32
        )
        if head == 0:
            total_buf[...] = product
        elif head < mine - 1:
            total_buf[...] += product
        else:
            o_ref[...] = (total_buf[...] + product).astype(BF16)

    for kind in range(3):
        for g in (1, 2):
            for d in range(1, TEAM):
                deal(kind, g, d).wait_send()
    for head in range(mine):
        for d in range(1, TEAM):
            for copy in home(d, head):
                copy.wait_send()
        for d in range(TEAM):
            twin(d, tp, head).wait_send()

    @pl.when(has_next)
    def _():
        for kind in (V, K):
            for s in range(TEAM):
                first_hop(kind, s).wait_send()
            for i in range(2):
                near_hop(kind, i).wait_send()

    @pl.when(edge_next & (me < TEAM - 1))
    def _():
        edge_hop(V).wait_send()

    @pl.when(edge_next)
    def _():
        edge_hop(K).wait_send()

    @pl.when(far_next)
    def _():
        relay_in().wait_send()

    @pl.when(relay_next)
    def _():
        relay_out().wait_send()

    @pl.when(has_prev2)
    def _():
        for s in range(TEAM):
            turn_hop(s).wait_send()

    @pl.when(middle)
    def _():
        for head in range(mine):
            for j in range(TEAM):
                part_hop(head, j).wait_send()
            stat_hop(head).wait_send()


def angle_tables(tokens, n_sp):
    inverse = ROPE_BASE ** (-np.arange(0, HEAD, 2) / HEAD)

    def pair(positions):
        angles = positions[:, None] * inverse[None, :]
        cosine, sine = np.cos(angles), np.sin(angles)
        return (
            np.concatenate([cosine, cosine], axis=1),
            np.concatenate([-sine, sine], axis=1),
        )

    by_group = []
    for stride in STRIDES:
        order = np.arange(tokens).reshape(tokens // stride, stride).T.reshape(-1)
        by_group.append(pair(order.astype(np.float64)))
    rows = np.stack([np.stack([t[i] for t in by_group]) for i in range(2)])
    base = np.zeros((n_sp, 8, HEAD))
    base[:, 0], base[:, 1] = pair(np.arange(n_sp) * float(tokens))
    return np.concatenate([rows.reshape(-1, HEAD), base.reshape(-1, HEAD)]).astype(np.float32)


def shards(n_sp, queries, keys, values, w_out):
    tokens, width = queries.shape[1:]
    heads = width // HEAD
    mine = heads // TEAM
    part = mine * HEAD
    span = TEAM * tokens
    angles = angle_tables(tokens, n_sp)
    any_spec = pl.BlockSpec(memory_space=pl.ANY)
    vmem = pl.BlockSpec(memory_space=pltpu.VMEM)
    dma = pltpu.SemaphoreType.DMA
    return pl.pallas_call(
        functools.partial(kernel, (tokens, n_sp, heads)),
        out_shape=jax.ShapeDtypeStruct((tokens, w_out.shape[1]), BF16),
        in_specs=[any_spec] * 5,
        out_specs=vmem,
        scratch_shapes=[
            pltpu.VMEM((3, 3, tokens, width), BF16),
            pltpu.VMEM((3, 3, tokens, width), BF16),
            pltpu.VMEM((2, mine, TEAM * HEAD, w_out.shape[1]), BF16),
            pltpu.VMEM(angles.shape, F32),
            pltpu.VMEM((2, 3, tokens, HEAD), F32),
            pltpu.VMEM((2, tokens, tokens), BF16),
            pltpu.VMEM((2, TEAM, tokens, part), BF16),
            pltpu.VMEM((TEAM, tokens, part), BF16),
            pltpu.VMEM((2, KEYS + tokens, width), BF16),
            pltpu.VMEM((2, 2 + TEAM, tokens, part), BF16),
            pltpu.VMEM((2, 2 * TEAM, tokens, part), BF16),
            pltpu.VMEM((KEYS, width), BF16),
            pltpu.VMEM((3, mine, span, HEAD), F32),
            pltpu.VMEM((3, mine, span, HEAD), F32),
            pltpu.VMEM((heads, tokens, HEAD), F32),
            pltpu.VMEM((heads, tokens, HEAD), F32),
            pltpu.VMEM((4, KEYS, 2 * KEYS), F32),
            pltpu.VMEM((mine, span, HEAD), BF16),
            pltpu.VMEM((mine, span // KEYS, KEYS), F32),
            pltpu.VMEM((mine, span, HEAD), BF16),
            pltpu.VMEM((mine, span // KEYS, KEYS), F32),
            pltpu.VMEM((mine, TEAM, tokens, HEAD), BF16),
            pltpu.VMEM((mine, TEAM, 8, KEYS), F32),
            pltpu.VMEM((mine, TEAM, tokens, HEAD), BF16),
            pltpu.VMEM((mine, TEAM, 8, KEYS), F32),
            pltpu.VMEM((2, mine, tokens, TEAM * HEAD), BF16),
            pltpu.VMEM((tokens, w_out.shape[1]), F32),
            dma((3, 3)),
            dma((2, mine, TEAM)),
            dma,
            dma((3, 2, TEAM)),
            dma((3, 2, TEAM)),
            dma((2, TEAM)),
            dma((2, TEAM)),
            dma((2, 2)),
            dma((2, 2)),
            dma((TEAM,)),
            dma((TEAM,)),
            dma((2,)),
            dma((2,)),
            dma((2,)),
            dma,
            dma((mine, TEAM)),
            dma((mine, TEAM)),
            dma((mine,)),
            dma((mine,)),
            dma((TEAM, mine)),
            dma((TEAM, mine)),
            dma((TEAM, mine)),
            dma((TEAM, mine)),
            dma((TEAM, mine)),
            dma((TEAM, mine)),
        ],
        compiler_params=pltpu.CompilerParams(
            collective_id=0, has_side_effects=True, vmem_limit_bytes=53 * 1024 * 1024
        ),
    )(queries, keys, values, w_out, jnp.asarray(angles))


def solution(mesh):
    return jax.shard_map(
        functools.partial(shards, mesh.shape["sp"]),
        mesh=mesh,
        in_specs=(P(None, "sp", "tp"), P(None, "sp", "tp"), P(None, "sp", "tp"), P(None, "tp")),
        out_specs=P("sp", "tp"),
        check_vma=False,
    )
```

```python
import functools

import jax
import jax.numpy as jnp
import numpy as np
from jax import lax
from jax.experimental import pallas as pl
from jax.experimental.pallas import tpu as pltpu
from jax.sharding import PartitionSpec as P

HEAD = 128
KEYS = 128
STRIDES = (1, 4, 16)
ROPE_BASE = 10000.0
MASKED = -1e30
TEAM = 4

MESH = pl.DeviceIdType.MESH
F32 = jnp.float32
BF16 = jnp.bfloat16
Q, K, V = 0, 1, 2


def kernel(
    cfg,
    q_in, k_in, v_in, w_in, angles_in,
    o_ref,
    raw, ready, q_home, w_buf, angles, tables, perms,
    q_buf, q_next, q_near, kv0, kv1, kv2, relay, acc, lse, acc1, lse1, bias,
    part_out, stat_out, part_in, stat_in, near_out, mark_out, near_in, mark_in,
    att, att_stat, back, back_stat, full, total_buf,
    in_sem, w_sem, angles_sem, deal_send, deal_recv, pair_recv, first_send, first_recv,
    turn_send, turn_recv, low_send, low_recv, edge_send, edge_recv, relay_send, relay_recv,
    part_send, part_recv, stat_recv, near_send, near_recv, mark_recv,
    ret_send, ret_recv, tag_recv, d2d_send, d2d_recv,
):
    tokens, n_sp, heads = cfg
    width = heads * HEAD
    mine = heads // TEAM
    part = mine * HEAD
    span = TEAM * tokens
    few = tokens // STRIDES[2]
    lot = TEAM * few
    chunks = tokens // KEYS
    low = KEYS * STRIDES[1] // tokens
    sp = lax.axis_index("sp")
    tp = lax.axis_index("tp")
    team = sp // TEAM
    me = lax.rem(sp, TEAM)
    has_next = sp + TEAM < n_sp
    has_prev = sp >= TEAM
    has_prev2 = sp >= 2 * TEAM
    middle = has_prev & has_next
    edge_next = sp + 1 < n_sp
    edge_prev = sp >= 1
    relay_next = (me == 0) & has_next

    def partner(d):
        if d == 0:
            return me
        if d == 1:
            return me + 1 - 2 * lax.rem(me, 2)
        if d == 2:
            return lax.rem(me + 2, TEAM)
        return TEAM - 1 - me

    def cols(head):
        return slice(head * HEAD, (head + 1) * HEAD)

    def lanes_of(j):
        return pl.ds(pl.multiple_of(j * part, part), part)

    inputs = (q_in, k_in, v_in)
    loads = {}

    def load(kind, g):
        if (kind, g) == (V, 0):
            target = kv0.at[1, pl.ds(KEYS, tokens)]
        else:
            target = raw.at[kind, g]
        copy = pltpu.make_async_copy(inputs[kind].at[g], target, in_sem.at[kind, g])
        copy.start()
        loads[kind, g] = copy

    load(V, 2)
    angles_copy = pltpu.make_async_copy(angles_in, angles, angles_sem)
    angles_copy.start()
    for kind, g in ((K, 2), (Q, 2), (V, 1), (K, 1), (V, 0), (K, 0), (Q, 1), (Q, 0)):
        load(kind, g)
    barrier = pltpu.get_barrier_semaphore()

    def greet(where, when=None):
        def signal():
            pl.semaphore_signal(barrier, inc=1, device_id=where, device_id_type=MESH)

        if when is None:
            signal()
        else:
            pl.when(when)(signal)

    for d in range(1, TEAM):
        greet({"sp": team * TEAM + partner(d)})
    greet({"tp": 1 - tp})
    far_next = edge_next & (me == TEAM - 1)
    far_prev = edge_prev & (me == 0)
    greet({"sp": sp + TEAM}, has_next)
    greet({"sp": sp - TEAM}, has_prev)
    greet({"sp": sp + 1}, far_next)
    greet({"sp": sp - 1}, far_prev)

    row = lax.broadcasted_iota(jnp.int32, (tokens, tokens), 0)
    col = lax.broadcasted_iota(jnp.int32, (tokens, tokens), 1)

    def sorter(g):
        each = tokens // STRIDES[g]
        origin = lax.rem(row, each) * STRIDES[g] + row // each
        perms[g - 1] = jnp.where(origin == col, 1.0, 0.0).astype(BF16)

    def make_tables(g):
        at = pl.multiple_of(6 * tokens + 8 * sp, 8)
        base = angles[pl.ds(at, 8), :]
        c0, s0 = base[0:1, :], base[1:2, :]
        c = angles[g * tokens : (g + 1) * tokens, :]
        s = angles[(3 + g) * tokens : (4 + g) * tokens, :]
        tables[0, g] = c0 * c - s0 * s
        tables[1, g] = s0 * c + c0 * s

    def turned(x, kind, g):
        x = x * tables[0, g] + pltpu.roll(x, HEAD // 2, 1) * tables[1, g]
        return x * HEAD ** (-0.5) if kind == Q else x

    def slot(kind, g, head, s):
        if kind == Q:
            return q_buf.at[g - 1, head, s]
        if g == 2:
            return kv2.at[kind - 1, head, TEAM + s]
        return kv1.at[kind - 1, head, s]

    def prepare(kind, g, d):
        j = partner(d)
        x = jnp.dot(perms[g - 1], raw[kind, g, :, lanes_of(j)], preferred_element_type=F32)
        for head in range(mine):
            y = x[:, cols(head)]
            if kind != V:
                y = turned(y, kind, g)
            target = slot(kind, g, head, me) if d == 0 else ready.at[kind, g - 1, j, head]
            target[...] = y.astype(BF16)

    def recv_of(kind, g, head, d):
        if g == 1 and kind != Q:
            return pair_recv.at[head]
        return deal_recv.at[kind if g == 2 else 3, head, d - 1]

    def deal(kind, g, head, d):
        return pltpu.make_async_remote_copy(
            src_ref=ready.at[kind, g - 1, partner(d), head],
            dst_ref=slot(kind, g, head, me),
            send_sem=deal_send,
            recv_sem=recv_of(kind, g, head, d),
            device_id={"sp": team * TEAM + partner(d)},
            device_id_type=MESH,
        )

    def settle(ref, sem):
        pltpu.make_async_copy(ref, ref, sem).wait()

    def onward(src, dst, send, recv, to):
        return pltpu.make_async_remote_copy(
            src_ref=src, dst_ref=dst, send_sem=send, recv_sem=recv,
            device_id={"sp": lax.rem(to + n_sp, n_sp)}, device_id_type=MESH,
        )

    def first_hop(kind, head, s):
        return onward(
            kv2.at[kind - 1, head, TEAM + s], kv2.at[kind - 1, head, s],
            first_send, first_recv.at[head], sp + TEAM,
        )

    def turn_hop(head, s):
        return onward(
            q_buf.at[1, head, s], q_next.at[head, s], turn_send, turn_recv.at[head], sp - TEAM,
        )

    def low_hop(head, s):
        return onward(
            q_buf.at[0, head, s], q_near.at[head, s], low_send, low_recv.at[head], sp - TEAM,
        )

    def edge_hop(kind):
        return onward(
            kv0.at[kind - 1, pl.ds(tokens, KEYS)], kv0.at[kind - 1, pl.ds(0, KEYS)],
            edge_send, edge_recv, sp + 1,
        )

    def relay_in():
        return onward(
            kv0.at[1, pl.ds(tokens, KEYS)], relay, edge_send, relay_recv, sp - (TEAM - 1),
        )

    def relay_out():
        return onward(relay, kv0.at[1, pl.ds(0, KEYS)], relay_send, edge_recv, sp + TEAM)

    def part_hop(head, j):
        rows = pl.ds(j * tokens, tokens)
        return onward(
            part_out.at[head, rows], part_in.at[head, rows],
            part_send.at[0], part_recv.at[head], sp + TEAM,
        )

    def stat_hop(head):
        return onward(
            stat_out.at[head], stat_in.at[head], part_send.at[1], stat_recv.at[head], sp + TEAM,
        )

    def near_hop(head):
        return onward(
            near_out.at[head], near_in.at[head, pl.ds(0, near_out.shape[1])],
            near_send.at[0], near_recv.at[head], sp + TEAM,
        )

    def mark_hop(head):
        return onward(
            mark_out.at[head], mark_in.at[head], near_send.at[1], mark_recv.at[head], sp + TEAM,
        )

    def forward(kind, g, head, s):
        if g == 2 and kind == Q:
            pl.when(has_prev2)(lambda: turn_hop(head, s).start())
        elif g == 2:
            pl.when(has_next)(lambda: first_hop(kind, head, s).start())
        elif kind == Q:
            pl.when(has_prev & (s < low))(lambda: low_hop(head, s).start())

    def arrive(kind, g, head):
        for d in (1, 2, 3):
            s = partner(d)
            settle(slot(kind, g, head, s), recv_of(kind, g, head, d))
            forward(kind, g, head, s)

    def send_first(kind, g, first=False):
        loads[kind, g].wait()
        for d in (3, 1, 2, 0):
            prepare(kind, g, d)
            if first and d == 3:
                count = TEAM
                for extra in (has_next, has_prev, far_next, far_prev):
                    count = count + extra.astype(jnp.int32)
                pl.semaphore_wait(barrier, count)
            if d:
                deal(kind, g, 0, d).start()
            else:
                forward(kind, g, 0, me)

    def send_rest(kinds, g):
        for head in range(1, mine):
            for kind in kinds:
                for d in (3, 1, 2):
                    deal(kind, g, head, d).start()
                forward(kind, g, head, me)

    def own(kind):
        loads[kind, 0].wait()

        def step(h, carry):
            lanes = pl.ds(pl.multiple_of(h * HEAD, HEAD), HEAD)
            x = turned(raw[kind, 0, :, lanes].astype(F32), kind, 0).astype(BF16)
            if kind == K:
                kv0[0, KEYS:, lanes] = x
            else:
                q_home[:, lanes] = x
            return carry

        lax.fori_loop(0, heads, step, 0, unroll=2)

    sorter(2)
    send_first(V, 2, first=True)
    for half in range(2):
        for head in range(mine):
            for s in range(TEAM):
                rows = pl.ds(half * width + s * part + head * HEAD, HEAD)
                copy = pltpu.make_async_copy(
                    w_in.at[rows],
                    w_buf.at[half, head, pl.ds(s * HEAD, HEAD)],
                    w_sem,
                )
                copy.start()
    angles_copy.wait()
    make_tables(2)
    send_first(K, 2)
    send_first(Q, 2)
    send_rest((V, K, Q), 2)
    sorter(1)
    send_first(V, 1)
    make_tables(1)
    arrive(V, 2, 0)
    send_first(Q, 1)
    send_first(K, 1)
    send_rest((V, Q, K), 1)
    arrive(K, 2, 0)
    make_tables(0)
    own(K)
    loads[V, 0].wait()

    @pl.when(edge_next & (me < TEAM - 1))
    def _():
        for kind in (V, K):
            edge_hop(kind).start()

    @pl.when(far_next)
    def _():
        relay_in().start()

    own(Q)

    @pl.when(jnp.logical_not(edge_prev))
    def _():
        for kind in range(2):
            kv0[kind, 0:KEYS, :] = jnp.zeros((KEYS, width), BF16)

    @pl.when(jnp.logical_not(has_prev))
    def _():
        for kind in range(2):
            for s in range(TEAM):
                for head in range(mine):
                    kv2[kind, head, s] = jnp.zeros((tokens, HEAD), BF16)
        for head in range(mine):
            near_in[head] = jnp.zeros((span, HEAD), BF16)
            mark_in[head] = jnp.full(mark_in.shape[1:], MASKED, F32)

    @pl.when(jnp.logical_not(has_prev2))
    def _():
        for head in range(mine):
            part_in[head] = jnp.zeros((span, HEAD), BF16)
            stat_in[head] = jnp.full(stat_in.shape[1:], MASKED, F32)

    @pl.when(has_prev)
    def _():
        for head in range(mine):
            near_in[head, low * tokens :] = jnp.zeros((span - low * tokens, HEAD), BF16)

    for head in range(mine):
        mark_out[head] = jnp.full(mark_out.shape[1:], MASKED, F32)

    def band(index):
        a = lax.broadcasted_iota(jnp.int32, (KEYS, 2 * KEYS), 0)
        b = lax.broadcasted_iota(jnp.int32, (KEYS, 2 * KEYS), 1)
        allowed = (b >= jnp.maximum(a, KEYS - index)) & (b <= a + KEYS)
        return jnp.where(allowed, 0.0, MASKED)

    bias[0] = band(sp * tokens)
    bias[1] = band(KEYS)
    a = lax.broadcasted_iota(jnp.int32, (lot, 2 * lot), 0)
    b = lax.broadcasted_iota(jnp.int32, (lot, 2 * lot), 1)
    start = jnp.where(has_prev, 0, lot)
    bias[2, 0:lot, 0 : 2 * lot] = jnp.where((b <= a + lot) & (b >= start), 0.0, MASKED)
    bias[2, lot : 2 * lot, 0 : 2 * lot] = jnp.where(b >= a, 0.0, MASKED)

    def attend(tiles):
        scores = [
            lax.dot_general(t[0], t[1], (((1,), (1,)), ((), ())), preferred_element_type=F32)
            + t[3]
            for t in tiles
        ]
        best = [jnp.max(x, axis=1, keepdims=True) for x in scores]
        weights = [jnp.exp(x - m) for x, m in zip(scores, best)]
        outs = [
            jnp.dot(p.astype(BF16), t[2], preferred_element_type=F32)
            for p, t in zip(weights, tiles)
        ]
        total = [jnp.sum(p, axis=1, keepdims=True) for p in weights]
        for t, out, m, l in zip(tiles, outs, best, total):
            out_ref, log_ref, index, where = t[4]
            out_ref[(*index, where)] = out / l
            log_ref[(*index, where)] = jnp.broadcast_to(m + jnp.log(l), out.shape)

    def group1(n):
        def step(i, carry):
            tiles = []
            for u in range(mine):
                h = i * mine + u
                lanes = pl.ds(pl.multiple_of(h * HEAD, HEAD), HEAD)
                rows = slice(n * KEYS, (n + 2) * KEYS)
                tiles.append((
                    q_home[n * KEYS : (n + 1) * KEYS, lanes],
                    kv0[0, rows, lanes], kv0[1, rows, lanes], bias[min(n, 1)],
                    (acc1, lse1, (h,), pl.ds(n * KEYS, KEYS)),
                ))
            attend(tiles)
            return carry

        lax.fori_loop(0, heads // mine, step, 0, unroll=2)

    each = tokens // STRIDES[1]
    pair = KEYS // each

    def band2(source, first, count, r):
        rows = slice(r * each, (r + 1) * each)
        return source[first : first + count, rows, :].reshape(count * each, HEAD)

    def group2():
        for i in range(TEAM // pair):
            first = max(i - 1, 0) * pair
            count = (i + 1) * pair - first
            for r in range(STRIDES[1]):
                where = pl.ds(r + STRIDES[1] * KEYS * i, KEYS, stride=STRIDES[1])
                tiles = []
                for head in range(mine):
                    tiles.append((
                        band2(q_buf.at[0, head], i * pair, pair, r),
                        band2(kv1.at[0, head], first, count, r),
                        band2(kv1.at[1, head], first, count, r),
                        bias[1, :, 2 * KEYS - count * each :],
                        (acc, lse, (0, head), where),
                    ))
                attend(tiles)

    def group2_next(head):
        tiles = []
        for r in range(STRIDES[1]):
            tiles.append((
                band2(q_near.at[head], 0, pair, r),
                band2(kv1.at[0, head], TEAM - pair, pair, r),
                band2(kv1.at[1, head], TEAM - pair, pair, r),
                bias[1, :, 0:KEYS],
                (acc, lse, (3, head), pl.ds(r, KEYS, stride=STRIDES[1])),
            ))
        attend(tiles)

    def group3(head, queries, count, off, which):
        for first in range(0, STRIDES[2], 4):
            tiles = []
            for r in range(first, first + 4):
                rows = slice(r * few, (r + 1) * few)
                query = queries[:, rows, :].reshape(lot, HEAD)
                key = kv2[0, head, 0:count, rows, :].reshape(count * few, HEAD)
                value = kv2[1, head, 0:count, rows, :].reshape(count * few, HEAD)
                where = pl.ds(r, lot, stride=STRIDES[2])
                tiles.append((query, key, value, off, (acc, lse, (which, head), where)))
            attend(tiles)

    eye = (
        lax.broadcasted_iota(jnp.int32, (KEYS, KEYS), 0)
        == lax.broadcasted_iota(jnp.int32, (KEYS, KEYS), 1)
    )

    def to_row(x):
        return jnp.sum(jnp.where(eye, x, 0.0), axis=0, keepdims=True)

    def to_col(x):
        return jnp.sum(jnp.where(eye, x, 0.0), axis=1, keepdims=True)

    def store_part(slot_at, head, c, out_ref, log_ref):
        rows = slice(c * KEYS, (c + 1) * KEYS)
        out_ref[head, rows] = acc[slot_at, head, rows, :].astype(BF16)
        log_ref[head, c : c + 1, :] = to_row(lse[slot_at, head, rows, :])

    def first_done(head):
        @pl.when(has_prev)
        def _():
            settle(kv2.at[:, head, pl.ds(0, TEAM)], first_recv.at[head])

    def pass_on(head):
        @pl.when(middle)
        def _():
            settle(q_next.at[head], turn_recv.at[head])
            group3(head, q_next.at[head], TEAM, bias[2, lot : 2 * lot, 0:lot], 2)

    def pass_send(head):
        @pl.when(middle)
        def _():
            for j in range(TEAM):
                for c in range(j * chunks, (j + 1) * chunks):
                    store_part(2, head, c, part_out, stat_out)
                part_hop(head, j).start()
            stat_hop(head).start()

    def here(head):
        group3(head, q_buf.at[1, head], 2 * TEAM, bias[2, 0:lot, 0 : 2 * lot], 1)

    def low_pass(head):
        settle(kv1.at[:, head, pl.ds(0, TEAM - 1)], pair_recv.at[head])

        @pl.when(has_next)
        def _():
            settle(q_near.at[head], low_recv.at[head])
            group2_next(head)
            for c in range(low * chunks):
                store_part(3, head, c, near_out, mark_out)
            near_hop(head).start()
            mark_hop(head).start()

    arrive(Q, 2, 0)
    group1(1)
    arrive(V, 2, 1)
    first_done(0)
    pass_on(0)
    arrive(K, 2, 1)
    pass_send(0)
    here(0)
    arrive(Q, 2, 1)
    first_done(1)
    arrive(Q, 1, 0)
    pass_on(1)
    pass_send(1)
    here(1)
    low_pass(0)
    arrive(Q, 1, 1)
    low_pass(1)

    group2()

    def merge(j, head, out_ref, log_ref):
        for c in range(chunks):
            rows = pl.ds(pl.multiple_of(j * tokens + c * KEYS, KEYS), KEYS)
            logs = [lse[g, head, rows, :] for g in range(2)]
            logs.append(to_col(stat_in[head, pl.ds(j * chunks + c, 1), :]))
            logs.append(to_col(mark_in[head, pl.ds(j * chunks + c, 1), :]))
            outs = [acc[g, head, rows, :] for g in range(2)]
            outs.append(part_in[head, rows, :].astype(F32))
            outs.append(near_in[head, rows, :].astype(F32))
            peak = jnp.maximum(jnp.maximum(logs[0], logs[1]), jnp.maximum(logs[2], logs[3]))
            scales = [jnp.exp(x - peak) for x in logs]
            lower = sum(scales)
            upper = sum(x * y for x, y in zip(scales, outs))
            out_ref[c * KEYS : (c + 1) * KEYS, :] = (upper / lower).astype(BF16)
            log_ref[c : c + 1, :] = to_row(peak + jnp.log(lower))

    def place_of(s):
        return pl.ds(pl.multiple_of(s * HEAD, HEAD), HEAD)

    def home(d, head):
        peer = partner(d)
        where = {"sp": team * TEAM + peer}
        return (
            pltpu.make_async_remote_copy(
                src_ref=att.at[head, peer], dst_ref=back.at[head, me],
                send_sem=ret_send.at[0], recv_sem=ret_recv.at[d - 1, head],
                device_id=where, device_id_type=MESH,
            ),
            pltpu.make_async_remote_copy(
                src_ref=att_stat.at[head, peer], dst_ref=back_stat.at[head, me],
                send_sem=ret_send.at[1], recv_sem=tag_recv.at[d - 1, head],
                device_id=where, device_id_type=MESH,
            ),
        )

    def wait_home(d, head):
        settle(back.at[head, partner(d)], ret_recv.at[d - 1, head])
        settle(back_stat.at[head, partner(d)], tag_recv.at[d - 1, head])

    def finish(d, head):
        s = partner(d)
        h = s * mine + head
        for c in range(chunks):
            rows = slice(c * KEYS, (c + 1) * KEYS)
            log_a = lse1[h, rows, :]
            log_b = to_col(back_stat[head, s, c : c + 1, :])
            peak = jnp.maximum(log_a, log_b)
            scale_a, scale_b = jnp.exp(log_a - peak), jnp.exp(log_b - peak)
            upper = scale_a * acc1[h, rows, :] + scale_b * back[head, s, rows, :].astype(F32)
            full[tp, head, rows, place_of(s)] = (upper / (scale_a + scale_b)).astype(BF16)

    def twin(d, half, head):
        here = full.at[half, head, :, place_of(partner(d))]
        return pltpu.make_async_remote_copy(
            src_ref=here, dst_ref=here,
            send_sem=d2d_send, recv_sem=d2d_recv.at[head],
            device_id={"tp": 1 - tp}, device_id_type=MESH,
        )

    pltpu.make_async_copy(w_buf, w_buf, w_sem).wait()
    for head in range(mine):

        @pl.when(has_prev2)
        def _():
            settle(stat_in.at[head], stat_recv.at[head])
            settle(part_in.at[head], part_recv.at[head])

        @pl.when(has_prev)
        def _():
            settle(mark_in.at[head], mark_recv.at[head])
            settle(near_in.at[head, pl.ds(0, near_out.shape[1])], near_recv.at[head])

        for d in (3, 1, 2, 0):
            j = partner(d)
            if d:
                merge(j, head, att.at[head, j], att_stat.at[head, j])
                for copy in home(d, head):
                    copy.start()
            else:
                merge(j, head, back.at[head, j], back_stat.at[head, j])

    @pl.when(far_next)
    def _():
        edge_hop(K).start()

    @pl.when(relay_next)
    def _():
        settle(relay, relay_recv)
        relay_out().start()

    @pl.when(edge_prev)
    def _():
        settle(kv0.at[:, pl.ds(0, KEYS)], edge_recv)

    group1(0)
    for head in range(mine):
        finish(0, head)
        twin(0, tp, head).start()
    for head in range(mine):
        for d in (1, 2, 3):
            wait_home(d, head)
            finish(d, head)
            twin(d, tp, head).start()
        product = jnp.dot(full[tp, head], w_buf[tp, head], preferred_element_type=F32)
        settle(full.at[1 - tp, head], d2d_recv.at[head])
        product = product + jnp.dot(
            full[1 - tp, head], w_buf[1 - tp, head], preferred_element_type=F32
        )
        if head == 0:
            total_buf[...] = product
        elif head < mine - 1:
            total_buf[...] += product
        else:
            o_ref[...] = (total_buf[...] + product).astype(BF16)

    settle(raw.at[:, :, pl.ds(0, tokens * 2 * (TEAM - 1) // (3 * TEAM))], deal_send)
    settle(back.at[:, pl.ds(0, TEAM - 1)], ret_send.at[0])
    settle(back_stat.at[:, pl.ds(0, TEAM - 1)], ret_send.at[1])
    settle(full.at[tp], d2d_send)

    @pl.when(has_next)
    def _():
        settle(kv2.at[:, :, pl.ds(TEAM, TEAM)], first_send)
        settle(near_out, near_send.at[0])
        settle(mark_out, near_send.at[1])

    @pl.when(edge_next)
    def _():
        settle(kv0.at[:, pl.ds(0, KEYS)], edge_send)

    @pl.when(relay_next)
    def _():
        settle(relay, relay_send)

    @pl.when(has_prev2)
    def _():
        settle(q_next, turn_send)

    @pl.when(has_prev)
    def _():
        settle(q_near, low_send)

    @pl.when(middle)
    def _():
        settle(part_out, part_send.at[0])
        settle(stat_out, part_send.at[1])


def angle_tables(tokens, n_sp):
    inverse = ROPE_BASE ** (-np.arange(0, HEAD, 2) / HEAD)

    def pair(positions):
        angles = positions[:, None] * inverse[None, :]
        cosine, sine = np.cos(angles), np.sin(angles)
        return (
            np.concatenate([cosine, cosine], axis=1),
            np.concatenate([-sine, sine], axis=1),
        )

    by_group = []
    for stride in STRIDES:
        order = np.arange(tokens).reshape(tokens // stride, stride).T.reshape(-1)
        by_group.append(pair(order.astype(np.float64)))
    rows = np.stack([np.stack([t[i] for t in by_group]) for i in range(2)])
    base = np.zeros((n_sp, 8, HEAD))
    base[:, 0], base[:, 1] = pair(np.arange(n_sp) * float(tokens))
    return np.concatenate([rows.reshape(-1, HEAD), base.reshape(-1, HEAD)]).astype(np.float32)


def shards(n_sp, queries, keys, values, w_out):
    tokens, width = queries.shape[1:]
    heads = width // HEAD
    mine = heads // TEAM
    part = mine * HEAD
    span = TEAM * tokens
    low = KEYS * STRIDES[1] // tokens
    angles = angle_tables(tokens, n_sp)
    any_spec = pl.BlockSpec(memory_space=pl.ANY)
    vmem = pl.BlockSpec(memory_space=pltpu.VMEM)
    dma = pltpu.SemaphoreType.DMA
    return pl.pallas_call(
        functools.partial(kernel, (tokens, n_sp, heads)),
        out_shape=jax.ShapeDtypeStruct((tokens, w_out.shape[1]), BF16),
        in_specs=[any_spec] * 5,
        out_specs=vmem,
        scratch_shapes=[
            pltpu.VMEM((3, 3, tokens, width), BF16),
            pltpu.VMEM((3, 2, TEAM, mine, tokens, HEAD), BF16),
            pltpu.VMEM((tokens, width), BF16),
            pltpu.VMEM((2, mine, TEAM * HEAD, w_out.shape[1]), BF16),
            pltpu.VMEM(angles.shape, F32),
            pltpu.VMEM((2, 3, tokens, HEAD), F32),
            pltpu.VMEM((2, tokens, tokens), BF16),
            pltpu.VMEM((2, mine, TEAM, tokens, HEAD), BF16),
            pltpu.VMEM((mine, TEAM, tokens, HEAD), BF16),
            pltpu.VMEM((mine, low, tokens, HEAD), BF16),
            pltpu.VMEM((2, KEYS + tokens, width), BF16),
            pltpu.VMEM((2, mine, TEAM, tokens, HEAD), BF16),
            pltpu.VMEM((2, mine, 2 * TEAM, tokens, HEAD), BF16),
            pltpu.VMEM((KEYS, width), BF16),
            pltpu.VMEM((4, mine, span, HEAD), F32),
            pltpu.VMEM((4, mine, span, HEAD), F32),
            pltpu.VMEM((heads, tokens, HEAD), F32),
            pltpu.VMEM((heads, tokens, HEAD), F32),
            pltpu.VMEM((3, KEYS, 2 * KEYS), F32),
            pltpu.VMEM((mine, span, HEAD), BF16),
            pltpu.VMEM((mine, span // KEYS, KEYS), F32),
            pltpu.VMEM((mine, span, HEAD), BF16),
            pltpu.VMEM((mine, span // KEYS, KEYS), F32),
            pltpu.VMEM((mine, low * tokens, HEAD), BF16),
            pltpu.VMEM((mine, span // KEYS, KEYS), F32),
            pltpu.VMEM((mine, span, HEAD), BF16),
            pltpu.VMEM((mine, span // KEYS, KEYS), F32),
            pltpu.VMEM((mine, TEAM, tokens, HEAD), BF16),
            pltpu.VMEM((mine, TEAM, 8, KEYS), F32),
            pltpu.VMEM((mine, TEAM, tokens, HEAD), BF16),
            pltpu.VMEM((mine, TEAM, 8, KEYS), F32),
            pltpu.VMEM((2, mine, tokens, TEAM * HEAD), BF16),
            pltpu.VMEM((tokens, w_out.shape[1]), F32),
            dma((3, 3)),
            dma,
            dma,
            dma,
            dma((4, mine, TEAM - 1)),
            dma((mine,)),
            dma,
            dma((mine,)),
            dma,
            dma((mine,)),
            dma,
            dma((mine,)),
            dma,
            dma,
            dma,
            dma,
            dma((2,)),
            dma((mine,)),
            dma((mine,)),
            dma((2,)),
            dma((mine,)),
            dma((mine,)),
            dma((2,)),
            dma((TEAM - 1, mine)),
            dma((TEAM - 1, mine)),
            dma,
            dma((mine,)),
        ],
        compiler_params=pltpu.CompilerParams(
            collective_id=0, has_side_effects=True, vmem_limit_bytes=53 * 1024 * 1024
        ),
    )(queries, keys, values, w_out, jnp.asarray(angles))


def solution(mesh):
    return jax.shard_map(
        functools.partial(shards, mesh.shape["sp"]),
        mesh=mesh,
        in_specs=(P(None, "sp", "tp"), P(None, "sp", "tp"), P(None, "sp", "tp"), P(None, "tp")),
        out_specs=P("sp", "tp"),
        check_vma=False,
    )
```

```python
import functools

import jax
import jax.numpy as jnp
import numpy as np
from jax import lax
from jax.experimental import pallas as pl
from jax.experimental.pallas import tpu as pltpu
from jax.sharding import PartitionSpec as P

HEAD = 128
KEYS = 128
STRIDES = (1, 4, 16)
ROPE_BASE = 10000.0
MASKED = -1e30
TEAM = 4

MESH = pl.DeviceIdType.MESH
F32 = jnp.float32
BF16 = jnp.bfloat16
Q, K, V = 0, 1, 2


def kernel(
    cfg,
    q_in, k_in, v_in, w_in, angles_in,
    o_ref,
    raw, ready, q_home, w_buf, angles, tables, perms,
    q_buf, q_next, q_near, kv0, kv1, kv2, relay, acc, lse, acc1, lse1, bias,
    part_out, stat_out, part_in, stat_in, near_out, mark_out, near_in, mark_in,
    att, att_stat, back, back_stat, full, total_buf,
    in_sem, w_sem, angles_sem, deal_send, deal_recv, pair_recv, first_send, first_recv,
    turn_send, turn_recv, low_send, low_recv, edge_send, edge_recv, relay_send, relay_recv,
    part_send, part_recv, stat_recv, near_send, near_recv, mark_recv,
    ret_send, ret_recv, tag_recv, d2d_send, d2d_recv,
):
    tokens, n_sp, heads = cfg
    width = heads * HEAD
    mine = heads // TEAM
    part = mine * HEAD
    span = TEAM * tokens
    few = tokens // STRIDES[2]
    lot = TEAM * few
    chunks = tokens // KEYS
    low = KEYS * STRIDES[1] // tokens
    sp = lax.axis_index("sp")
    tp = lax.axis_index("tp")
    team = sp // TEAM
    me = lax.rem(sp, TEAM)
    has_next = sp + TEAM < n_sp
    has_prev = sp >= TEAM
    has_prev2 = sp >= 2 * TEAM
    middle = has_prev & has_next
    edge_next = sp + 1 < n_sp
    edge_prev = sp >= 1
    relay_next = (me == 0) & has_next

    def partner(d):
        if d == 0:
            return me
        if d == 1:
            return me + 1 - 2 * lax.rem(me, 2)
        if d == 2:
            return lax.rem(me + 2, TEAM)
        return TEAM - 1 - me

    def cols(head):
        return slice(head * HEAD, (head + 1) * HEAD)

    def lanes_of(j):
        return pl.ds(pl.multiple_of(j * part, part), part)

    inputs = (q_in, k_in, v_in)
    loads = {}

    def load(kind, g):
        if (kind, g) == (V, 0):
            target = kv0.at[1, pl.ds(KEYS, tokens)]
        else:
            target = raw.at[kind, g]
        copy = pltpu.make_async_copy(inputs[kind].at[g], target, in_sem.at[kind, g])
        copy.start()
        loads[kind, g] = copy

    load(V, 2)
    angles_copy = pltpu.make_async_copy(angles_in, angles, angles_sem)
    angles_copy.start()
    for kind, g in ((K, 2), (Q, 2), (V, 1), (K, 1), (V, 0), (K, 0), (Q, 1), (Q, 0)):
        load(kind, g)
    barrier = pltpu.get_barrier_semaphore()

    def greet(where, when=None):
        def signal():
            pl.semaphore_signal(barrier, inc=1, device_id=where, device_id_type=MESH)

        if when is None:
            signal()
        else:
            pl.when(when)(signal)

    for d in range(1, TEAM):
        greet({"sp": team * TEAM + partner(d)})
    greet({"tp": 1 - tp})
    far_next = edge_next & (me == TEAM - 1)
    far_prev = edge_prev & (me == 0)
    greet({"sp": sp + TEAM}, has_next)
    greet({"sp": sp - TEAM}, has_prev)
    greet({"sp": sp + 1}, far_next)
    greet({"sp": sp - 1}, far_prev)

    row = lax.broadcasted_iota(jnp.int32, (tokens, tokens), 0)
    col = lax.broadcasted_iota(jnp.int32, (tokens, tokens), 1)

    def sorter(g):
        each = tokens // STRIDES[g]
        origin = lax.rem(row, each) * STRIDES[g] + row // each
        perms[g - 1] = jnp.where(origin == col, 1.0, 0.0).astype(BF16)

    def make_tables(g):
        at = pl.multiple_of(6 * tokens + 8 * sp, 8)
        base = angles[pl.ds(at, 8), :]
        c0, s0 = base[0:1, :], base[1:2, :]
        c = angles[g * tokens : (g + 1) * tokens, :]
        s = angles[(3 + g) * tokens : (4 + g) * tokens, :]
        tables[0, g] = c0 * c - s0 * s
        tables[1, g] = s0 * c + c0 * s

    def turned(x, kind, g):
        x = x * tables[0, g] + pltpu.roll(x, HEAD // 2, 1) * tables[1, g]
        return x * HEAD ** (-0.5) if kind == Q else x

    def slot(kind, g, head, s):
        if kind == Q:
            return q_buf.at[g - 1, head, s]
        if g == 2:
            return kv2.at[kind - 1, head, TEAM + s]
        return kv1.at[kind - 1, head, s]

    def prepare(kind, g, d):
        j = partner(d)
        x = jnp.dot(perms[g - 1], raw[kind, g, :, lanes_of(j)], preferred_element_type=F32)
        for head in range(mine):
            y = x[:, cols(head)]
            if kind != V:
                y = turned(y, kind, g)
            target = slot(kind, g, head, me) if d == 0 else ready.at[kind, g - 1, j, head]
            target[...] = y.astype(BF16)

    def recv_of(kind, g, head, d):
        if g == 1 and kind != Q:
            return pair_recv.at[head]
        return deal_recv.at[kind if g == 2 else 3, head, d - 1]

    def deal(kind, g, head, d):
        return pltpu.make_async_remote_copy(
            src_ref=ready.at[kind, g - 1, partner(d), head],
            dst_ref=slot(kind, g, head, me),
            send_sem=deal_send,
            recv_sem=recv_of(kind, g, head, d),
            device_id={"sp": team * TEAM + partner(d)},
            device_id_type=MESH,
        )

    def settle(ref, sem):
        pltpu.make_async_copy(ref, ref, sem).wait()

    def onward(src, dst, send, recv, to):
        return pltpu.make_async_remote_copy(
            src_ref=src, dst_ref=dst, send_sem=send, recv_sem=recv,
            device_id={"sp": lax.rem(to + n_sp, n_sp)}, device_id_type=MESH,
        )

    def first_hop(kind, head, s):
        return onward(
            kv2.at[kind - 1, head, TEAM + s], kv2.at[kind - 1, head, s],
            first_send, first_recv.at[head], sp + TEAM,
        )

    def turn_hop(head, s):
        return onward(
            q_buf.at[1, head, s], q_next.at[head, s], turn_send, turn_recv.at[head], sp - TEAM,
        )

    def low_hop(head, s):
        return onward(
            q_buf.at[0, head, s], q_near.at[head, s], low_send, low_recv.at[head], sp - TEAM,
        )

    def edge_hop(kind):
        return onward(
            kv0.at[kind - 1, pl.ds(tokens, KEYS)], kv0.at[kind - 1, pl.ds(0, KEYS)],
            edge_send, edge_recv, sp + 1,
        )

    def relay_in():
        return onward(
            kv0.at[1, pl.ds(tokens, KEYS)], relay, edge_send, relay_recv, sp - (TEAM - 1),
        )

    def relay_out():
        return onward(relay, kv0.at[1, pl.ds(0, KEYS)], relay_send, edge_recv, sp + TEAM)

    def part_hop(head, j):
        rows = pl.ds(j * tokens, tokens)
        return onward(
            part_out.at[head, rows], part_in.at[head, rows],
            part_send.at[0], part_recv.at[head], sp + TEAM,
        )

    def stat_hop(head):
        return onward(
            stat_out.at[head], stat_in.at[head], part_send.at[1], stat_recv.at[head], sp + TEAM,
        )

    def near_hop(head):
        return onward(
            near_out.at[head], near_in.at[head, pl.ds(0, near_out.shape[1])],
            near_send.at[0], near_recv.at[head], sp + TEAM,
        )

    def mark_hop(head):
        return onward(
            mark_out.at[head], mark_in.at[head], near_send.at[1], mark_recv.at[head], sp + TEAM,
        )

    def forward(kind, g, head, s):
        if g == 2 and kind == Q:
            pl.when(has_prev2)(lambda: turn_hop(head, s).start())
        elif g == 2:
            pl.when(has_next)(lambda: first_hop(kind, head, s).start())
        elif kind == Q:
            pl.when(has_prev & (s < low))(lambda: low_hop(head, s).start())

    def arrive(kind, g, head):
        for d in (1, 2, 3):
            s = partner(d)
            settle(slot(kind, g, head, s), recv_of(kind, g, head, d))
            forward(kind, g, head, s)

    def send_first(kind, g, first=False):
        loads[kind, g].wait()
        for d in (3, 1, 2, 0):
            prepare(kind, g, d)
            if first and d == 3:
                count = TEAM
                for extra in (has_next, has_prev, far_next, far_prev):
                    count = count + extra.astype(jnp.int32)
                pl.semaphore_wait(barrier, count)
            if d:
                deal(kind, g, 0, d).start()
            else:
                forward(kind, g, 0, me)

    def send_rest(kinds, g):
        for head in range(1, mine):
            for kind in kinds:
                for d in (3, 1, 2):
                    deal(kind, g, head, d).start()
                forward(kind, g, head, me)

    def own(kind):
        loads[kind, 0].wait()

        def step(h, carry):
            lanes = pl.ds(pl.multiple_of(h * HEAD, HEAD), HEAD)
            x = turned(raw[kind, 0, :, lanes].astype(F32), kind, 0).astype(BF16)
            if kind == K:
                kv0[0, KEYS:, lanes] = x
            else:
                q_home[:, lanes] = x
            return carry

        lax.fori_loop(0, heads, step, 0, unroll=2)

    sorter(2)
    send_first(V, 2, first=True)
    for half in range(2):
        for head in range(mine):
            for s in range(TEAM):
                rows = pl.ds(half * width + s * part + head * HEAD, HEAD)
                copy = pltpu.make_async_copy(
                    w_in.at[rows],
                    w_buf.at[half, head, pl.ds(s * HEAD, HEAD)],
                    w_sem,
                )
                copy.start()
    angles_copy.wait()
    make_tables(2)
    send_first(K, 2)
    send_first(Q, 2)
    send_rest((V, K, Q), 2)
    sorter(1)
    send_first(V, 1)
    make_tables(1)
    arrive(V, 2, 0)
    send_first(Q, 1)
    send_first(K, 1)
    send_rest((V, Q, K), 1)
    arrive(K, 2, 0)
    make_tables(0)
    own(K)
    loads[V, 0].wait()

    @pl.when(edge_next & (me < TEAM - 1))
    def _():
        for kind in (V, K):
            edge_hop(kind).start()

    @pl.when(far_next)
    def _():
        relay_in().start()

    own(Q)

    @pl.when(jnp.logical_not(edge_prev))
    def _():
        for kind in range(2):
            kv0[kind, 0:KEYS, :] = jnp.zeros((KEYS, width), BF16)

    @pl.when(jnp.logical_not(has_prev))
    def _():
        for kind in range(2):
            for s in range(TEAM):
                for head in range(mine):
                    kv2[kind, head, s] = jnp.zeros((tokens, HEAD), BF16)
        for head in range(mine):
            near_in[head] = jnp.zeros((span, HEAD), BF16)
            mark_in[head] = jnp.full(mark_in.shape[1:], MASKED, F32)

    @pl.when(jnp.logical_not(has_prev2))
    def _():
        for head in range(mine):
            part_in[head] = jnp.zeros((span, HEAD), BF16)
            stat_in[head] = jnp.full(stat_in.shape[1:], MASKED, F32)

    @pl.when(has_prev)
    def _():
        for head in range(mine):
            near_in[head, low * tokens :] = jnp.zeros((span - low * tokens, HEAD), BF16)

    for head in range(mine):
        mark_out[head] = jnp.full(mark_out.shape[1:], MASKED, F32)

    def band(index):
        a = lax.broadcasted_iota(jnp.int32, (KEYS, 2 * KEYS), 0)
        b = lax.broadcasted_iota(jnp.int32, (KEYS, 2 * KEYS), 1)
        allowed = (b >= jnp.maximum(a, KEYS - index)) & (b <= a + KEYS)
        return jnp.where(allowed, 0.0, MASKED)

    bias[0] = band(sp * tokens)
    bias[1] = band(KEYS)
    a = lax.broadcasted_iota(jnp.int32, (lot, 2 * lot), 0)
    b = lax.broadcasted_iota(jnp.int32, (lot, 2 * lot), 1)
    start = jnp.where(has_prev, 0, lot)
    bias[2, 0:lot, 0 : 2 * lot] = jnp.where((b <= a + lot) & (b >= start), 0.0, MASKED)
    bias[2, lot : 2 * lot, 0 : 2 * lot] = jnp.where(b >= a, 0.0, MASKED)

    def attend(tiles):
        scores = [
            lax.dot_general(t[0], t[1], (((1,), (1,)), ((), ())), preferred_element_type=F32)
            + t[3]
            for t in tiles
        ]
        best = [jnp.max(x, axis=1, keepdims=True) for x in scores]
        weights = [jnp.exp(x - m) for x, m in zip(scores, best)]
        outs = [
            jnp.dot(p.astype(BF16), t[2], preferred_element_type=F32)
            for p, t in zip(weights, tiles)
        ]
        total = [jnp.sum(p, axis=1, keepdims=True) for p in weights]
        for t, out, m, l in zip(tiles, outs, best, total):
            out_ref, log_ref, index, where = t[4]
            out_ref[(*index, where)] = out / l
            log_ref[(*index, where)] = jnp.broadcast_to(m + jnp.log(l), out.shape)

    def group1(n):
        def step(i, carry):
            tiles = []
            for u in range(mine):
                h = i * mine + u
                lanes = pl.ds(pl.multiple_of(h * HEAD, HEAD), HEAD)
                rows = slice(n * KEYS, (n + 2) * KEYS)
                tiles.append((
                    q_home[n * KEYS : (n + 1) * KEYS, lanes],
                    kv0[0, rows, lanes], kv0[1, rows, lanes], bias[min(n, 1)],
                    (acc1, lse1, (h,), pl.ds(n * KEYS, KEYS)),
                ))
            attend(tiles)
            return carry

        lax.fori_loop(0, heads // mine, step, 0, unroll=2)

    each = tokens // STRIDES[1]
    pair = KEYS // each

    def band2(source, first, count, r):
        rows = slice(r * each, (r + 1) * each)
        return source[first : first + count, rows, :].reshape(count * each, HEAD)

    def group2():
        for i in range(TEAM // pair):
            first = max(i - 1, 0) * pair
            count = (i + 1) * pair - first
            for r in range(STRIDES[1]):
                where = pl.ds(r + STRIDES[1] * KEYS * i, KEYS, stride=STRIDES[1])
                tiles = []
                for head in range(mine):
                    tiles.append((
                        band2(q_buf.at[0, head], i * pair, pair, r),
                        band2(kv1.at[0, head], first, count, r),
                        band2(kv1.at[1, head], first, count, r),
                        bias[1, :, 2 * KEYS - count * each :],
                        (acc, lse, (0, head), where),
                    ))
                attend(tiles)

    def group2_next(head):
        tiles = []
        for r in range(STRIDES[1]):
            tiles.append((
                band2(q_near.at[head], 0, pair, r),
                band2(kv1.at[0, head], TEAM - pair, pair, r),
                band2(kv1.at[1, head], TEAM - pair, pair, r),
                bias[1, :, 0:KEYS],
                (acc, lse, (3, head), pl.ds(r, KEYS, stride=STRIDES[1])),
            ))
        attend(tiles)

    def group3(head, queries, count, off, which):
        for first in range(0, STRIDES[2], 4):
            tiles = []
            for r in range(first, first + 4):
                rows = slice(r * few, (r + 1) * few)
                query = queries[:, rows, :].reshape(lot, HEAD)
                key = kv2[0, head, 0:count, rows, :].reshape(count * few, HEAD)
                value = kv2[1, head, 0:count, rows, :].reshape(count * few, HEAD)
                where = pl.ds(r, lot, stride=STRIDES[2])
                tiles.append((query, key, value, off, (acc, lse, (which, head), where)))
            attend(tiles)

    eye = (
        lax.broadcasted_iota(jnp.int32, (KEYS, KEYS), 0)
        == lax.broadcasted_iota(jnp.int32, (KEYS, KEYS), 1)
    )

    def to_row(x):
        return jnp.sum(jnp.where(eye, x, 0.0), axis=0, keepdims=True)

    def to_col(x):
        return jnp.sum(jnp.where(eye, x, 0.0), axis=1, keepdims=True)

    def store_part(slot_at, head, c, out_ref, log_ref):
        rows = slice(c * KEYS, (c + 1) * KEYS)
        out_ref[head, rows] = acc[slot_at, head, rows, :].astype(BF16)
        log_ref[head, c : c + 1, :] = to_row(lse[slot_at, head, rows, :])

    def first_done(head):
        @pl.when(has_prev)
        def _():
            settle(kv2.at[:, head, pl.ds(0, TEAM)], first_recv.at[head])

    def pass_on(head):
        @pl.when(middle)
        def _():
            settle(q_next.at[head], turn_recv.at[head])
            group3(head, q_next.at[head], TEAM, bias[2, lot : 2 * lot, 0:lot], 2)

    def pass_send(head):
        @pl.when(middle)
        def _():
            for j in range(TEAM):
                for c in range(j * chunks, (j + 1) * chunks):
                    store_part(2, head, c, part_out, stat_out)
                part_hop(head, j).start()
            stat_hop(head).start()

    def here(head):
        group3(head, q_buf.at[1, head], 2 * TEAM, bias[2, 0:lot, 0 : 2 * lot], 1)

    def low_pass(head):
        settle(kv1.at[:, head, pl.ds(0, TEAM - 1)], pair_recv.at[head])

        @pl.when(has_next)
        def _():
            settle(q_near.at[head], low_recv.at[head])
            group2_next(head)
            for c in range(low * chunks):
                store_part(3, head, c, near_out, mark_out)
            near_hop(head).start()
            mark_hop(head).start()

    arrive(Q, 2, 0)
    group1(1)
    arrive(V, 2, 1)
    first_done(0)
    pass_on(0)
    arrive(K, 2, 1)
    pass_send(0)
    here(0)
    arrive(Q, 2, 1)
    first_done(1)
    arrive(Q, 1, 0)
    pass_on(1)
    pass_send(1)
    here(1)
    low_pass(0)
    arrive(Q, 1, 1)
    low_pass(1)

    group2()

    def merge(j, head, out_ref, log_ref):
        for c in range(chunks):
            rows = pl.ds(pl.multiple_of(j * tokens + c * KEYS, KEYS), KEYS)
            logs = [lse[g, head, rows, :] for g in range(2)]
            logs.append(to_col(stat_in[head, pl.ds(j * chunks + c, 1), :]))
            logs.append(to_col(mark_in[head, pl.ds(j * chunks + c, 1), :]))
            outs = [acc[g, head, rows, :] for g in range(2)]
            outs.append(part_in[head, rows, :].astype(F32))
            outs.append(near_in[head, rows, :].astype(F32))
            peak = jnp.maximum(jnp.maximum(logs[0], logs[1]), jnp.maximum(logs[2], logs[3]))
            scales = [jnp.exp(x - peak) for x in logs]
            lower = sum(scales)
            upper = sum(x * y for x, y in zip(scales, outs))
            out_ref[c * KEYS : (c + 1) * KEYS, :] = (upper / lower).astype(BF16)
            log_ref[c : c + 1, :] = to_row(peak + jnp.log(lower))

    def place_of(s):
        return pl.ds(pl.multiple_of(s * HEAD, HEAD), HEAD)

    def home(d, head):
        peer = partner(d)
        where = {"sp": team * TEAM + peer}
        return (
            pltpu.make_async_remote_copy(
                src_ref=att.at[head, peer], dst_ref=back.at[head, me],
                send_sem=ret_send.at[0], recv_sem=ret_recv.at[d - 1, head],
                device_id=where, device_id_type=MESH,
            ),
            pltpu.make_async_remote_copy(
                src_ref=att_stat.at[head, peer], dst_ref=back_stat.at[head, me],
                send_sem=ret_send.at[1], recv_sem=tag_recv.at[d - 1, head],
                device_id=where, device_id_type=MESH,
            ),
        )

    def wait_home(d, head):
        settle(back.at[head, partner(d)], ret_recv.at[d - 1, head])
        settle(back_stat.at[head, partner(d)], tag_recv.at[d - 1, head])

    def finish(d, head):
        s = partner(d)
        h = s * mine + head
        for c in range(chunks):
            rows = slice(c * KEYS, (c + 1) * KEYS)
            log_a = lse1[h, rows, :]
            log_b = to_col(back_stat[head, s, c : c + 1, :])
            peak = jnp.maximum(log_a, log_b)
            scale_a, scale_b = jnp.exp(log_a - peak), jnp.exp(log_b - peak)
            upper = scale_a * acc1[h, rows, :] + scale_b * back[head, s, rows, :].astype(F32)
            full[tp, head, rows, place_of(s)] = (upper / (scale_a + scale_b)).astype(BF16)

    def twin(d, half, head):
        here = full.at[half, head, :, place_of(partner(d))]
        return pltpu.make_async_remote_copy(
            src_ref=here, dst_ref=here,
            send_sem=d2d_send, recv_sem=d2d_recv.at[head],
            device_id={"tp": 1 - tp}, device_id_type=MESH,
        )

    pltpu.make_async_copy(w_buf, w_buf, w_sem).wait()
    for head in range(mine):

        @pl.when(has_prev2)
        def _():
            settle(stat_in.at[head], stat_recv.at[head])
            settle(part_in.at[head], part_recv.at[head])

        @pl.when(has_prev)
        def _():
            settle(mark_in.at[head], mark_recv.at[head])
            settle(near_in.at[head, pl.ds(0, near_out.shape[1])], near_recv.at[head])

        for d in (3, 1, 2, 0):
            j = partner(d)
            if d:
                merge(j, head, att.at[head, j], att_stat.at[head, j])
                for copy in home(d, head):
                    copy.start()
            else:
                merge(j, head, back.at[head, j], back_stat.at[head, j])

    @pl.when(far_next)
    def _():
        edge_hop(K).start()

    @pl.when(relay_next)
    def _():
        settle(relay, relay_recv)
        relay_out().start()

    @pl.when(edge_prev)
    def _():
        settle(kv0.at[:, pl.ds(0, KEYS)], edge_recv)

    group1(0)
    for head in range(mine):
        finish(0, head)
        twin(0, tp, head).start()
    def mixed(half, head):
        return jnp.dot(full[half, head], w_buf[half, head], preferred_element_type=F32)

    for head in range(mine):
        for d in (3, 2, 1):
            wait_home(d, head)
            finish(d, head)
            twin(d, tp, head).start()
        if head:
            total_buf[...] += mixed(tp, head)
        else:
            total_buf[...] = mixed(tp, head)
        settle(full.at[1 - tp, head], d2d_recv.at[head])
        if head < mine - 1:
            total_buf[...] += mixed(1 - tp, head)
        else:
            o_ref[...] = (total_buf[...] + mixed(1 - tp, head)).astype(BF16)

    settle(raw.at[:, :, pl.ds(0, tokens * 2 * (TEAM - 1) // (3 * TEAM))], deal_send)
    settle(back.at[:, pl.ds(0, TEAM - 1)], ret_send.at[0])
    settle(back_stat.at[:, pl.ds(0, TEAM - 1)], ret_send.at[1])
    settle(full.at[tp], d2d_send)

    @pl.when(has_next)
    def _():
        settle(kv2.at[:, :, pl.ds(TEAM, TEAM)], first_send)
        settle(near_out, near_send.at[0])
        settle(mark_out, near_send.at[1])

    @pl.when(edge_next)
    def _():
        settle(kv0.at[:, pl.ds(0, KEYS)], edge_send)

    @pl.when(relay_next)
    def _():
        settle(relay, relay_send)

    @pl.when(has_prev2)
    def _():
        settle(q_next, turn_send)

    @pl.when(has_prev)
    def _():
        settle(q_near, low_send)

    @pl.when(middle)
    def _():
        settle(part_out, part_send.at[0])
        settle(stat_out, part_send.at[1])


def angle_tables(tokens, n_sp):
    inverse = ROPE_BASE ** (-np.arange(0, HEAD, 2) / HEAD)

    def pair(positions):
        angles = positions[:, None] * inverse[None, :]
        cosine, sine = np.cos(angles), np.sin(angles)
        return (
            np.concatenate([cosine, cosine], axis=1),
            np.concatenate([-sine, sine], axis=1),
        )

    by_group = []
    for stride in STRIDES:
        order = np.arange(tokens).reshape(tokens // stride, stride).T.reshape(-1)
        by_group.append(pair(order.astype(np.float64)))
    rows = np.stack([np.stack([t[i] for t in by_group]) for i in range(2)])
    base = np.zeros((n_sp, 8, HEAD))
    base[:, 0], base[:, 1] = pair(np.arange(n_sp) * float(tokens))
    return np.concatenate([rows.reshape(-1, HEAD), base.reshape(-1, HEAD)]).astype(np.float32)


def shards(n_sp, queries, keys, values, w_out):
    tokens, width = queries.shape[1:]
    heads = width // HEAD
    mine = heads // TEAM
    part = mine * HEAD
    span = TEAM * tokens
    low = KEYS * STRIDES[1] // tokens
    angles = angle_tables(tokens, n_sp)
    any_spec = pl.BlockSpec(memory_space=pl.ANY)
    vmem = pl.BlockSpec(memory_space=pltpu.VMEM)
    dma = pltpu.SemaphoreType.DMA
    return pl.pallas_call(
        functools.partial(kernel, (tokens, n_sp, heads)),
        out_shape=jax.ShapeDtypeStruct((tokens, w_out.shape[1]), BF16),
        in_specs=[any_spec] * 5,
        out_specs=vmem,
        scratch_shapes=[
            pltpu.VMEM((3, 3, tokens, width), BF16),
            pltpu.VMEM((3, 2, TEAM, mine, tokens, HEAD), BF16),
            pltpu.VMEM((tokens, width), BF16),
            pltpu.VMEM((2, mine, TEAM * HEAD, w_out.shape[1]), BF16),
            pltpu.VMEM(angles.shape, F32),
            pltpu.VMEM((2, 3, tokens, HEAD), F32),
            pltpu.VMEM((2, tokens, tokens), BF16),
            pltpu.VMEM((2, mine, TEAM, tokens, HEAD), BF16),
            pltpu.VMEM((mine, TEAM, tokens, HEAD), BF16),
            pltpu.VMEM((mine, low, tokens, HEAD), BF16),
            pltpu.VMEM((2, KEYS + tokens, width), BF16),
            pltpu.VMEM((2, mine, TEAM, tokens, HEAD), BF16),
            pltpu.VMEM((2, mine, 2 * TEAM, tokens, HEAD), BF16),
            pltpu.VMEM((KEYS, width), BF16),
            pltpu.VMEM((4, mine, span, HEAD), F32),
            pltpu.VMEM((4, mine, span, HEAD), F32),
            pltpu.VMEM((heads, tokens, HEAD), F32),
            pltpu.VMEM((heads, tokens, HEAD), F32),
            pltpu.VMEM((3, KEYS, 2 * KEYS), F32),
            pltpu.VMEM((mine, span, HEAD), BF16),
            pltpu.VMEM((mine, span // KEYS, KEYS), F32),
            pltpu.VMEM((mine, span, HEAD), BF16),
            pltpu.VMEM((mine, span // KEYS, KEYS), F32),
            pltpu.VMEM((mine, low * tokens, HEAD), BF16),
            pltpu.VMEM((mine, span // KEYS, KEYS), F32),
            pltpu.VMEM((mine, span, HEAD), BF16),
            pltpu.VMEM((mine, span // KEYS, KEYS), F32),
            pltpu.VMEM((mine, TEAM, tokens, HEAD), BF16),
            pltpu.VMEM((mine, TEAM, 8, KEYS), F32),
            pltpu.VMEM((mine, TEAM, tokens, HEAD), BF16),
            pltpu.VMEM((mine, TEAM, 8, KEYS), F32),
            pltpu.VMEM((2, mine, tokens, TEAM * HEAD), BF16),
            pltpu.VMEM((tokens, w_out.shape[1]), F32),
            dma((3, 3)),
            dma,
            dma,
            dma,
            dma((4, mine, TEAM - 1)),
            dma((mine,)),
            dma,
            dma((mine,)),
            dma,
            dma((mine,)),
            dma,
            dma((mine,)),
            dma,
            dma,
            dma,
            dma,
            dma((2,)),
            dma((mine,)),
            dma((mine,)),
            dma((2,)),
            dma((mine,)),
            dma((mine,)),
            dma((2,)),
            dma((TEAM - 1, mine)),
            dma((TEAM - 1, mine)),
            dma,
            dma((mine,)),
        ],
        compiler_params=pltpu.CompilerParams(
            collective_id=0, has_side_effects=True, vmem_limit_bytes=53 * 1024 * 1024
        ),
    )(queries, keys, values, w_out, jnp.asarray(angles))


def solution(mesh):
    return jax.shard_map(
        functools.partial(shards, mesh.shape["sp"]),
        mesh=mesh,
        in_specs=(P(None, "sp", "tp"), P(None, "sp", "tp"), P(None, "sp", "tp"), P(None, "tp")),
        out_specs=P("sp", "tp"),
        check_vma=False,
    )
```

```python
import functools

import jax
import jax.numpy as jnp
import numpy as np
from jax import lax
from jax.experimental import pallas as pl
from jax.experimental.pallas import tpu as pltpu
from jax.sharding import PartitionSpec as P

HEAD = 128
KEYS = 128
STRIDES = (1, 4, 16)
ROPE_BASE = 10000.0
MASKED = -1e30
TEAM = 4
TAGS = 16

MESH = pl.DeviceIdType.MESH
F32 = jnp.float32
BF16 = jnp.bfloat16
Q, K, V = 0, 1, 2


def kernel(
    cfg,
    q_in, k_in, v_in, w_in, angles_in,
    o_ref,
    raw, ready, q_home, w_buf, angles, tables, perms,
    q_buf, q_next, q_near, kv0, kv1, kv2, relay, acc, lse, acc1, lse1, bias,
    part_out, stat_out, part_in, stat_in, near_out, mark_out, near_in, mark_in,
    att, back, full, total_buf,
    in_sem, w_sem, angles_sem, deal_send, deal_recv, low_deal, pair_recv, first_send, first_recv,
    turn_send, turn_recv, low_send, low_recv, edge_send, edge_recv, relay_send, relay_recv,
    part_send, part_recv, stat_recv, near_send, near_recv, mark_recv,
    ret_send, ret_recv, d2d_send, d2d_recv,
):
    tokens, n_sp, heads = cfg
    width = heads * HEAD
    mine = heads // TEAM
    part = mine * HEAD
    span = TEAM * tokens
    few = tokens // STRIDES[2]
    lot = TEAM * few
    chunks = tokens // KEYS
    low = KEYS * STRIDES[1] // tokens
    sp = lax.axis_index("sp")
    tp = lax.axis_index("tp")
    team = sp // TEAM
    me = lax.rem(sp, TEAM)
    has_next = sp + TEAM < n_sp
    has_prev = sp >= TEAM
    has_prev2 = sp >= 2 * TEAM
    middle = has_prev & has_next
    edge_next = sp + 1 < n_sp
    edge_prev = sp >= 1
    relay_next = (me == 0) & has_next

    def partner(d):
        if d == 0:
            return me
        if d == 1:
            return me + 1 - 2 * lax.rem(me, 2)
        if d == 2:
            return lax.rem(me + 2, TEAM)
        return TEAM - 1 - me

    def cols(head):
        return slice(head * HEAD, (head + 1) * HEAD)

    def lanes_of(j):
        return pl.ds(pl.multiple_of(j * part, part), part)

    inputs = (q_in, k_in, v_in)
    loads = {}

    def load(kind, g):
        if (kind, g) == (V, 0):
            target = kv0.at[1, pl.ds(KEYS, tokens)]
        else:
            target = raw.at[kind, g]
        copy = pltpu.make_async_copy(inputs[kind].at[g], target, in_sem.at[kind, g])
        copy.start()
        loads[kind, g] = copy

    load(V, 2)
    angles_copy = pltpu.make_async_copy(angles_in, angles, angles_sem)
    angles_copy.start()
    for kind, g in ((K, 2), (Q, 2), (V, 1), (K, 1), (V, 0), (K, 0), (Q, 1), (Q, 0)):
        load(kind, g)
    barrier = pltpu.get_barrier_semaphore()

    def greet(where, when=None):
        def signal():
            pl.semaphore_signal(barrier, inc=1, device_id=where, device_id_type=MESH)

        if when is None:
            signal()
        else:
            pl.when(when)(signal)

    for d in range(1, TEAM):
        greet({"sp": team * TEAM + partner(d)})
    greet({"tp": 1 - tp})
    far_next = edge_next & (me == TEAM - 1)
    far_prev = edge_prev & (me == 0)
    greet({"sp": sp + TEAM}, has_next)
    greet({"sp": sp - TEAM}, has_prev)
    greet({"sp": sp + 1}, far_next)
    greet({"sp": sp - 1}, far_prev)

    row = lax.broadcasted_iota(jnp.int32, (tokens, tokens), 0)
    col = lax.broadcasted_iota(jnp.int32, (tokens, tokens), 1)

    def sorter(g):
        each = tokens // STRIDES[g]
        origin = lax.rem(row, each) * STRIDES[g] + row // each
        perms[g - 1] = jnp.where(origin == col, 1.0, 0.0).astype(BF16)

    def make_tables(g):
        at = pl.multiple_of(6 * tokens + 8 * sp, 8)
        base = angles[pl.ds(at, 8), :]
        c0, s0 = base[0:1, :], base[1:2, :]
        c = angles[g * tokens : (g + 1) * tokens, :]
        s = angles[(3 + g) * tokens : (4 + g) * tokens, :]
        tables[0, g] = c0 * c - s0 * s
        tables[1, g] = s0 * c + c0 * s

    def turned(x, kind, g):
        x = x * tables[0, g] + pltpu.roll(x, HEAD // 2, 1) * tables[1, g]
        return x * HEAD ** (-0.5) if kind == Q else x

    def slot(kind, g, head, s):
        if kind == Q:
            return q_buf.at[g - 1, head, s]
        if g == 2:
            return kv2.at[kind - 1, head, TEAM + s]
        return kv1.at[kind - 1, head, s]

    def prepare(kind, g, d):
        j = partner(d)
        x = jnp.dot(perms[g - 1], raw[kind, g, :, lanes_of(j)], preferred_element_type=F32)
        for head in range(mine):
            y = x[:, cols(head)]
            if kind != V:
                y = turned(y, kind, g)
            target = slot(kind, g, head, me) if d == 0 else ready.at[kind, g - 1, j, head]
            target[...] = y.astype(BF16)

    def recv_of(kind, g, head, d):
        if g == 1 and kind != Q:
            return pair_recv.at[head]
        if g == 1:
            return low_deal.at[head]
        return deal_recv.at[kind, head, d - 1]

    def deal(kind, g, head, d):
        return pltpu.make_async_remote_copy(
            src_ref=ready.at[kind, g - 1, partner(d), head],
            dst_ref=slot(kind, g, head, me),
            send_sem=deal_send,
            recv_sem=recv_of(kind, g, head, d),
            device_id={"sp": team * TEAM + partner(d)},
            device_id_type=MESH,
        )

    def settle(ref, sem):
        pltpu.make_async_copy(ref, ref, sem).wait()

    def onward(src, dst, send, recv, to):
        return pltpu.make_async_remote_copy(
            src_ref=src, dst_ref=dst, send_sem=send, recv_sem=recv,
            device_id={"sp": lax.rem(to + n_sp, n_sp)}, device_id_type=MESH,
        )

    def first_hop(kind, head, s):
        return onward(
            kv2.at[kind - 1, head, TEAM + s], kv2.at[kind - 1, head, s],
            first_send, first_recv.at[head], sp + TEAM,
        )

    def turn_hop(head, s):
        return onward(
            q_buf.at[1, head, s], q_next.at[head, s], turn_send, turn_recv.at[head], sp - TEAM,
        )

    def low_hop(head, s):
        return onward(
            q_buf.at[0, head, s], q_near.at[head, s], low_send, low_recv.at[head], sp - TEAM,
        )

    def edge_hop(kind):
        return onward(
            kv0.at[kind - 1, pl.ds(tokens, KEYS)], kv0.at[kind - 1, pl.ds(0, KEYS)],
            edge_send, edge_recv, sp + 1,
        )

    def relay_in():
        return onward(
            kv0.at[1, pl.ds(tokens, KEYS)], relay, edge_send, relay_recv, sp - (TEAM - 1),
        )

    def relay_out():
        return onward(relay, kv0.at[1, pl.ds(0, KEYS)], relay_send, edge_recv, sp + TEAM)

    def part_hop(head, j):
        rows = pl.ds(j * tokens, tokens)
        return onward(
            part_out.at[head, rows], part_in.at[head, rows],
            part_send.at[0], part_recv.at[head], sp + TEAM,
        )

    def stat_hop(head):
        return onward(
            stat_out.at[head], stat_in.at[head], part_send.at[1], stat_recv.at[head], sp + TEAM,
        )

    def near_hop(head):
        return onward(
            near_out.at[head], near_in.at[head, pl.ds(0, near_out.shape[1])],
            near_send.at[0], near_recv.at[head], sp + TEAM,
        )

    def mark_hop(head):
        return onward(
            mark_out.at[head], mark_in.at[head], near_send.at[1], mark_recv.at[head], sp + TEAM,
        )

    def forward(kind, g, head, s):
        if g == 2 and kind == Q:
            pl.when(has_prev2)(lambda: turn_hop(head, s).start())
        elif g == 2:
            pl.when(has_next)(lambda: first_hop(kind, head, s).start())
        elif kind == Q:
            pl.when(has_prev & (s < low))(lambda: low_hop(head, s).start())

    def arrive(kind, g, head):
        if g == 1:
            settle(q_buf.at[0, head, pl.ds(0, TEAM - 1)], low_deal.at[head])
        for d in (1, 2, 3):
            s = partner(d)
            if g == 2:
                settle(slot(kind, g, head, s), recv_of(kind, g, head, d))
            forward(kind, g, head, s)

    def send_first(kind, g, first=False):
        loads[kind, g].wait()
        for d in (3, 1, 2, 0):
            prepare(kind, g, d)
            if first and d == 3:
                count = TEAM
                for extra in (has_next, has_prev, far_next, far_prev):
                    count = count + extra.astype(jnp.int32)
                pl.semaphore_wait(barrier, count)
            if d:
                deal(kind, g, 0, d).start()
            else:
                forward(kind, g, 0, me)

    def send_rest(kinds, g):
        for head in range(1, mine):
            for kind in kinds:
                for d in (3, 1, 2):
                    deal(kind, g, head, d).start()
                forward(kind, g, head, me)

    def own(kind):
        loads[kind, 0].wait()

        def step(h, carry):
            lanes = pl.ds(pl.multiple_of(h * HEAD, HEAD), HEAD)
            x = turned(raw[kind, 0, :, lanes].astype(F32), kind, 0).astype(BF16)
            if kind == K:
                kv0[0, KEYS:, lanes] = x
            else:
                q_home[:, lanes] = x
            return carry

        lax.fori_loop(0, heads, step, 0, unroll=2)

    sorter(2)
    send_first(V, 2, first=True)
    for half in range(2):
        for head in range(mine):
            for s in range(TEAM):
                rows = pl.ds(half * width + s * part + head * HEAD, HEAD)
                copy = pltpu.make_async_copy(
                    w_in.at[rows],
                    w_buf.at[half, head, pl.ds(s * HEAD, HEAD)],
                    w_sem,
                )
                copy.start()
    angles_copy.wait()
    make_tables(2)
    send_first(K, 2)
    send_first(Q, 2)
    send_rest((V, K, Q), 2)
    sorter(1)
    send_first(V, 1)
    make_tables(1)
    arrive(V, 2, 0)
    send_first(Q, 1)
    send_first(K, 1)
    send_rest((V, Q, K), 1)
    arrive(K, 2, 0)
    make_tables(0)
    own(K)
    loads[V, 0].wait()

    @pl.when(edge_next & (me < TEAM - 1))
    def _():
        for kind in (K, V):
            edge_hop(kind).start()

    @pl.when(far_next)
    def _():
        relay_in().start()

    own(Q)

    @pl.when(jnp.logical_not(edge_prev))
    def _():
        for kind in range(2):
            kv0[kind, 0:KEYS, :] = jnp.zeros((KEYS, width), BF16)

    @pl.when(jnp.logical_not(has_prev))
    def _():
        for kind in range(2):
            for s in range(TEAM):
                for head in range(mine):
                    kv2[kind, head, s] = jnp.zeros((tokens, HEAD), BF16)
        for head in range(mine):
            near_in[head] = jnp.zeros((span, HEAD), BF16)
            mark_in[head] = jnp.full(mark_in.shape[1:], MASKED, F32)

    @pl.when(jnp.logical_not(has_prev2))
    def _():
        for head in range(mine):
            part_in[head] = jnp.zeros((span, HEAD), BF16)
            stat_in[head] = jnp.full(stat_in.shape[1:], MASKED, F32)

    @pl.when(has_prev)
    def _():
        for head in range(mine):
            near_in[head, low * tokens :] = jnp.zeros((span - low * tokens, HEAD), BF16)

    for head in range(mine):
        mark_out[head] = jnp.full(mark_out.shape[1:], MASKED, F32)

    def band(index):
        a = lax.broadcasted_iota(jnp.int32, (KEYS, 2 * KEYS), 0)
        b = lax.broadcasted_iota(jnp.int32, (KEYS, 2 * KEYS), 1)
        allowed = (b >= jnp.maximum(a, KEYS - index)) & (b <= a + KEYS)
        return jnp.where(allowed, 0.0, MASKED)

    bias[0] = band(sp * tokens)
    bias[1] = band(KEYS)
    a = lax.broadcasted_iota(jnp.int32, (lot, 2 * lot), 0)
    b = lax.broadcasted_iota(jnp.int32, (lot, 2 * lot), 1)
    start = jnp.where(has_prev, 0, lot)
    bias[2, 0:lot, 0 : 2 * lot] = jnp.where((b <= a + lot) & (b >= start), 0.0, MASKED)
    bias[2, lot : 2 * lot, 0 : 2 * lot] = jnp.where(b >= a, 0.0, MASKED)

    def attend(tiles):
        scores = [
            lax.dot_general(t[0], t[1], (((1,), (1,)), ((), ())), preferred_element_type=F32)
            + t[3]
            for t in tiles
        ]
        best = [jnp.max(x, axis=1, keepdims=True) for x in scores]
        weights = [jnp.exp(x - m) for x, m in zip(scores, best)]
        outs = [
            jnp.dot(p.astype(BF16), t[2], preferred_element_type=F32)
            for p, t in zip(weights, tiles)
        ]
        total = [jnp.sum(p, axis=1, keepdims=True) for p in weights]
        for t, out, m, l in zip(tiles, outs, best, total):
            out_ref, log_ref, index, where = t[4]
            out_ref[(*index, where)] = out / l
            log_ref[(*index, where)] = jnp.broadcast_to(m + jnp.log(l), out.shape)

    def group1(n):
        def step(i, carry):
            tiles = []
            for u in range(mine):
                h = i * mine + u
                lanes = pl.ds(pl.multiple_of(h * HEAD, HEAD), HEAD)
                rows = slice(n * KEYS, (n + 2) * KEYS)
                tiles.append((
                    q_home[n * KEYS : (n + 1) * KEYS, lanes],
                    kv0[0, rows, lanes], kv0[1, rows, lanes], bias[min(n, 1)],
                    (acc1, lse1, (h,), pl.ds(n * KEYS, KEYS)),
                ))
            attend(tiles)
            return carry

        lax.fori_loop(0, heads // mine, step, 0, unroll=2)

    each = tokens // STRIDES[1]
    pair = KEYS // each

    def band2(source, first, count, r):
        rows = slice(r * each, (r + 1) * each)
        return source[first : first + count, rows, :].reshape(count * each, HEAD)

    def group2():
        for i in range(TEAM // pair):
            first = max(i - 1, 0) * pair
            count = (i + 1) * pair - first
            for r in range(STRIDES[1]):
                where = pl.ds(r + STRIDES[1] * KEYS * i, KEYS, stride=STRIDES[1])
                tiles = []
                for head in range(mine):
                    tiles.append((
                        band2(q_buf.at[0, head], i * pair, pair, r),
                        band2(kv1.at[0, head], first, count, r),
                        band2(kv1.at[1, head], first, count, r),
                        bias[1, :, 2 * KEYS - count * each :],
                        (acc, lse, (0, head), where),
                    ))
                attend(tiles)

    def group2_next(head):
        tiles = []
        for r in range(STRIDES[1]):
            tiles.append((
                band2(q_near.at[head], 0, pair, r),
                band2(kv1.at[0, head], TEAM - pair, pair, r),
                band2(kv1.at[1, head], TEAM - pair, pair, r),
                bias[1, :, 0:KEYS],
                (acc, lse, (3, head), pl.ds(r, KEYS, stride=STRIDES[1])),
            ))
        attend(tiles)

    def group3(head, queries, count, off, which):
        for first in range(0, STRIDES[2], 4):
            tiles = []
            for r in range(first, first + 4):
                rows = slice(r * few, (r + 1) * few)
                query = queries[:, rows, :].reshape(lot, HEAD)
                key = kv2[0, head, 0:count, rows, :].reshape(count * few, HEAD)
                value = kv2[1, head, 0:count, rows, :].reshape(count * few, HEAD)
                where = pl.ds(r, lot, stride=STRIDES[2])
                tiles.append((query, key, value, off, (acc, lse, (which, head), where)))
            attend(tiles)

    eye = (
        lax.broadcasted_iota(jnp.int32, (KEYS, KEYS), 0)
        == lax.broadcasted_iota(jnp.int32, (KEYS, KEYS), 1)
    )

    def to_row(x):
        return jnp.sum(jnp.where(eye, x, 0.0), axis=0, keepdims=True)

    def to_col(x):
        return jnp.sum(jnp.where(eye, x, 0.0), axis=1, keepdims=True)

    def store_part(slot_at, head, c, out_ref, log_ref):
        rows = slice(c * KEYS, (c + 1) * KEYS)
        out_ref[head, rows] = acc[slot_at, head, rows, :].astype(BF16)
        log_ref[head, c : c + 1, :] = to_row(lse[slot_at, head, rows, :])

    def first_done(head):
        @pl.when(has_prev)
        def _():
            settle(kv2.at[:, head, pl.ds(0, TEAM)], first_recv.at[head])

    def pass_on(head):
        @pl.when(middle)
        def _():
            settle(q_next.at[head], turn_recv.at[head])
            group3(head, q_next.at[head], TEAM, bias[2, lot : 2 * lot, 0:lot], 2)

    def pass_send(head):
        @pl.when(middle)
        def _():
            for j in range(TEAM):
                for c in range(j * chunks, (j + 1) * chunks):
                    store_part(2, head, c, part_out, stat_out)
                part_hop(head, j).start()
            stat_hop(head).start()

    def local(head):
        group3(head, q_buf.at[1, head], 2 * TEAM, bias[2, 0:lot, 0 : 2 * lot], 1)

    def low_pass(head):
        settle(kv1.at[:, head, pl.ds(0, TEAM - 1)], pair_recv.at[head])

        @pl.when(has_next)
        def _():
            settle(q_near.at[head], low_recv.at[head])
            group2_next(head)
            for c in range(low * chunks):
                store_part(3, head, c, near_out, mark_out)
            near_hop(head).start()
            mark_hop(head).start()

    arrive(Q, 2, 0)
    group1(1)
    arrive(V, 2, 1)
    first_done(0)
    pass_on(0)
    arrive(K, 2, 1)
    pass_send(0)
    local(0)
    arrive(Q, 2, 1)
    first_done(1)
    arrive(Q, 1, 0)
    pass_on(1)
    pass_send(1)
    local(1)
    low_pass(0)
    arrive(Q, 1, 1)
    low_pass(1)

    group2()

    tag_row = lax.broadcasted_iota(jnp.int32, (TAGS, KEYS), 0)

    def merge(j, head, out_ref):
        tags = jnp.zeros((TAGS, KEYS), F32)
        for c in range(chunks):
            rows = pl.ds(pl.multiple_of(j * tokens + c * KEYS, KEYS), KEYS)
            logs = [lse[g, head, rows, :] for g in range(2)]
            logs.append(to_col(stat_in[head, pl.ds(j * chunks + c, 1), :]))
            logs.append(to_col(mark_in[head, pl.ds(j * chunks + c, 1), :]))
            outs = [acc[g, head, rows, :] for g in range(2)]
            outs.append(part_in[head, rows, :].astype(F32))
            outs.append(near_in[head, rows, :].astype(F32))
            peak = jnp.maximum(jnp.maximum(logs[0], logs[1]), jnp.maximum(logs[2], logs[3]))
            scales = [jnp.exp(x - peak) for x in logs]
            lower = sum(scales)
            upper = sum(x * y for x, y in zip(scales, outs))
            out_ref[c * KEYS : (c + 1) * KEYS, :] = (upper / lower).astype(BF16)
            rest = to_row(peak + jnp.log(lower))
            for i in range(3):
                piece = rest.astype(BF16).astype(F32)
                tags = jnp.where(tag_row == 3 * c + i, piece, tags)
                rest = rest - piece
        out_ref[tokens:, :] = tags.astype(BF16)

    def place_of(s):
        return pl.ds(pl.multiple_of(s * HEAD, HEAD), HEAD)

    def home(d, head):
        peer = partner(d)
        return pltpu.make_async_remote_copy(
            src_ref=att.at[head, peer], dst_ref=back.at[head, me],
            send_sem=ret_send, recv_sem=ret_recv.at[d - 1, head],
            device_id={"sp": team * TEAM + peer}, device_id_type=MESH,
        )

    def wait_home(d, head):
        settle(back.at[head, partner(d)], ret_recv.at[d - 1, head])

    def finish(d, head):
        s = partner(d)
        h = s * mine + head
        tags = back[head, s, tokens:, :].astype(F32)
        for c in range(chunks):
            rows = slice(c * KEYS, (c + 1) * KEYS)
            log_a = lse1[h, rows, :]
            log_b = to_col(jnp.sum(jnp.where(tag_row // 3 == c, tags, 0.0), axis=0, keepdims=True))
            peak = jnp.maximum(log_a, log_b)
            scale_a, scale_b = jnp.exp(log_a - peak), jnp.exp(log_b - peak)
            upper = scale_a * acc1[h, rows, :] + scale_b * back[head, s, rows, :].astype(F32)
            full[tp, head, rows, place_of(s)] = (upper / (scale_a + scale_b)).astype(BF16)

    def twin(d, half, head):
        here = full.at[half, head, :, place_of(partner(d))]
        return pltpu.make_async_remote_copy(
            src_ref=here, dst_ref=here,
            send_sem=d2d_send, recv_sem=d2d_recv.at[head],
            device_id={"tp": 1 - tp}, device_id_type=MESH,
        )

    pltpu.make_async_copy(w_buf, w_buf, w_sem).wait()
    for head in range(mine):

        @pl.when(has_prev2)
        def _():
            settle(stat_in.at[head], stat_recv.at[head])
            settle(part_in.at[head], part_recv.at[head])

        @pl.when(has_prev)
        def _():
            settle(mark_in.at[head], mark_recv.at[head])
            settle(near_in.at[head, pl.ds(0, near_out.shape[1])], near_recv.at[head])

        for d in (1, 3, 2, 0):
            j = partner(d)
            if d:
                merge(j, head, att.at[head, j])
                home(d, head).start()
            else:
                merge(j, head, back.at[head, j])

    @pl.when(far_next)
    def _():
        edge_hop(K).start()

    @pl.when(relay_next)
    def _():
        settle(relay, relay_recv)
        relay_out().start()

    @pl.when(edge_prev)
    def _():
        settle(kv0.at[:, pl.ds(0, KEYS)], edge_recv)

    group1(0)
    for head in range(mine):
        finish(0, head)
        twin(0, tp, head).start()
    def mixed(half, head):
        return jnp.dot(full[half, head], w_buf[half, head], preferred_element_type=F32)

    for head in range(mine):
        for d in (1, 2, 3):
            wait_home(d, head)
            finish(d, head)
            twin(d, tp, head).start()
        if head == 0:
            total_buf[...] = mixed(tp, head)
    for head in range(mine):
        if head:
            total_buf[...] += mixed(tp, head)
        settle(full.at[1 - tp, head], d2d_recv.at[head])
        if head < mine - 1:
            total_buf[...] += mixed(1 - tp, head)
        else:
            o_ref[...] = (total_buf[...] + mixed(1 - tp, head)).astype(BF16)

    settle(raw.at[:, :, pl.ds(0, tokens * 2 * (TEAM - 1) // (3 * TEAM))], deal_send)
    settle(back.at[:, pl.ds(0, TEAM - 1)], ret_send)
    settle(full.at[tp], d2d_send)

    @pl.when(has_next)
    def _():
        settle(kv2.at[:, :, pl.ds(TEAM, TEAM)], first_send)
        settle(near_out, near_send.at[0])
        settle(mark_out, near_send.at[1])

    @pl.when(edge_next)
    def _():
        settle(kv0.at[:, pl.ds(0, KEYS)], edge_send)

    @pl.when(relay_next)
    def _():
        settle(relay, relay_send)

    @pl.when(has_prev2)
    def _():
        settle(q_next, turn_send)

    @pl.when(has_prev)
    def _():
        settle(q_near, low_send)

    @pl.when(middle)
    def _():
        settle(part_out, part_send.at[0])
        settle(stat_out, part_send.at[1])


def angle_tables(tokens, n_sp):
    inverse = ROPE_BASE ** (-np.arange(0, HEAD, 2) / HEAD)

    def pair(positions):
        angles = positions[:, None] * inverse[None, :]
        cosine, sine = np.cos(angles), np.sin(angles)
        return (
            np.concatenate([cosine, cosine], axis=1),
            np.concatenate([-sine, sine], axis=1),
        )

    by_group = []
    for stride in STRIDES:
        order = np.arange(tokens).reshape(tokens // stride, stride).T.reshape(-1)
        by_group.append(pair(order.astype(np.float64)))
    rows = np.stack([np.stack([t[i] for t in by_group]) for i in range(2)])
    base = np.zeros((n_sp, 8, HEAD))
    base[:, 0], base[:, 1] = pair(np.arange(n_sp) * float(tokens))
    return np.concatenate([rows.reshape(-1, HEAD), base.reshape(-1, HEAD)]).astype(np.float32)


def shards(n_sp, queries, keys, values, w_out):
    tokens, width = queries.shape[1:]
    heads = width // HEAD
    mine = heads // TEAM
    part = mine * HEAD
    span = TEAM * tokens
    low = KEYS * STRIDES[1] // tokens
    angles = angle_tables(tokens, n_sp)
    any_spec = pl.BlockSpec(memory_space=pl.ANY)
    vmem = pl.BlockSpec(memory_space=pltpu.VMEM)
    dma = pltpu.SemaphoreType.DMA
    return pl.pallas_call(
        functools.partial(kernel, (tokens, n_sp, heads)),
        out_shape=jax.ShapeDtypeStruct((tokens, w_out.shape[1]), BF16),
        in_specs=[any_spec] * 5,
        out_specs=vmem,
        scratch_shapes=[
            pltpu.VMEM((3, 3, tokens, width), BF16),
            pltpu.VMEM((3, 2, TEAM, mine, tokens, HEAD), BF16),
            pltpu.VMEM((tokens, width), BF16),
            pltpu.VMEM((2, mine, TEAM * HEAD, w_out.shape[1]), BF16),
            pltpu.VMEM(angles.shape, F32),
            pltpu.VMEM((2, 3, tokens, HEAD), F32),
            pltpu.VMEM((2, tokens, tokens), BF16),
            pltpu.VMEM((2, mine, TEAM, tokens, HEAD), BF16),
            pltpu.VMEM((mine, TEAM, tokens, HEAD), BF16),
            pltpu.VMEM((mine, low, tokens, HEAD), BF16),
            pltpu.VMEM((2, KEYS + tokens, width), BF16),
            pltpu.VMEM((2, mine, TEAM, tokens, HEAD), BF16),
            pltpu.VMEM((2, mine, 2 * TEAM, tokens, HEAD), BF16),
            pltpu.VMEM((KEYS, width), BF16),
            pltpu.VMEM((4, mine, span, HEAD), F32),
            pltpu.VMEM((4, mine, span, HEAD), F32),
            pltpu.VMEM((heads, tokens, HEAD), F32),
            pltpu.VMEM((heads, tokens, HEAD), F32),
            pltpu.VMEM((3, KEYS, 2 * KEYS), F32),
            pltpu.VMEM((mine, span, HEAD), BF16),
            pltpu.VMEM((mine, span // KEYS, KEYS), F32),
            pltpu.VMEM((mine, span, HEAD), BF16),
            pltpu.VMEM((mine, span // KEYS, KEYS), F32),
            pltpu.VMEM((mine, low * tokens, HEAD), BF16),
            pltpu.VMEM((mine, span // KEYS, KEYS), F32),
            pltpu.VMEM((mine, span, HEAD), BF16),
            pltpu.VMEM((mine, span // KEYS, KEYS), F32),
            pltpu.VMEM((mine, TEAM, tokens + TAGS, HEAD), BF16),
            pltpu.VMEM((mine, TEAM, tokens + TAGS, HEAD), BF16),
            pltpu.VMEM((2, mine, tokens, TEAM * HEAD), BF16),
            pltpu.VMEM((tokens, w_out.shape[1]), F32),
            dma((3, 3)),
            dma,
            dma,
            dma,
            dma((3, mine, TEAM - 1)),
            dma((mine,)),
            dma((mine,)),
            dma,
            dma((mine,)),
            dma,
            dma((mine,)),
            dma,
            dma((mine,)),
            dma,
            dma,
            dma,
            dma,
            dma((2,)),
            dma((mine,)),
            dma((mine,)),
            dma((2,)),
            dma((mine,)),
            dma((mine,)),
            dma,
            dma((TEAM - 1, mine)),
            dma,
            dma((mine,)),
        ],
        compiler_params=pltpu.CompilerParams(
            collective_id=0, has_side_effects=True, vmem_limit_bytes=53 * 1024 * 1024
        ),
    )(queries, keys, values, w_out, jnp.asarray(angles))


def solution(mesh):
    return jax.shard_map(
        functools.partial(shards, mesh.shape["sp"]),
        mesh=mesh,
        in_specs=(P(None, "sp", "tp"), P(None, "sp", "tp"), P(None, "sp", "tp"), P(None, "tp")),
        out_specs=P("sp", "tp"),
        check_vma=False,
    )
```
